32 devices in a mesh: sp: 8 (over z, y), tp: 4 (over x, core).
Axes of the slice: x: 2, y: 2, z: 4, core: 2. Of those that a mesh axis runs over, the one named last changes fastest.
Arguments:
- latent: bfloat16 [1024, 4096], P(('sp', 'tp')), may hold values from -8 to 8
- context: bfloat16 [256, 4096], P('sp'), may hold values from -6 to 6
- condition: float32 [4096], P('sp'), may hold values from -6 to 6
- context_condition: float32 [4096], P('sp'), may hold values from -6 to 6
- shift_weight: bfloat16 [4096, 4096], P('sp', 'tp'), may hold values from -0.09375 to 0.09375
- scale_weight: bfloat16 [4096, 4096], P('sp', 'tp'), may hold values from -0.09375 to 0.09375
- gate_weight: bfloat16 [4096, 4096], P('sp', 'tp'), may hold values from -0.09375 to 0.09375
- norm_gain: float32 [4096], replicated, may hold values from 0.1 to 1.9
- decay_down: bfloat16 [4096, 128], replicated, may hold values from -0.09375 to 0.09375
- decay_up: bfloat16 [128, 4096], P(None, 'tp'), may hold values from -0.5 to 0.5
- rate_down: bfloat16 [4096, 128], replicated, may hold values from -0.09375 to 0.09375
- rate_up: bfloat16 [128, 4096], P(None, 'tp'), may hold values from -0.5 to 0.5
- head_bias: float32 [2, 4096], P(None, 'tp'), may hold values from -12 to 1
- query_weight: bfloat16 [4096, 4096], P(None, 'tp'), may hold values from -0.09375 to 0.09375
- key_weight: bfloat16 [4096, 4096], P(None, 'tp'), may hold values from -0.09375 to 0.09375
- value_weight: bfloat16 [4096, 4096], P(None, 'tp'), may hold values from -0.09375 to 0.09375
- branch_weight: bfloat16 [4096, 4096], P(None, 'tp'), may hold values from -0.09375 to 0.09375
- group_gain: float32 [4096], P('tp'), may hold values from 0.1 to 1.9
- out_weight: bfloat16 [4096, 4096], P('tp'), may hold values from -0.09375 to 0.09375
Outputs:
- updated: bfloat16 [1024, 4096], P(('sp', 'tp'))
The draws below stay inside these ranges and needn't reach their ends.
All inputs are finite; a program needn't handle non-finite values.
Results may differ from the reference program's by a relative error of at most 0.017.
Values may be sent and summed in bfloat16 or wider, within the bound.
A program may use at most 192 MiB of HBM per device.

```python
import math
import jax
import jax.numpy as jnp
from jax import lax

D = 4096
HEAD_DIM = 64
RANK = 128
TOKENS = 1024
CONTEXT = 256
N_TP = 4


def draw_latent(key, part):
    base_key = jax.random.fold_in(key, 11)
    shared = jax.random.normal(jax.random.fold_in(base_key, 2), (TOKENS // 64, 1, D), jnp.float32)
    shared = jnp.broadcast_to(shared, (TOKENS // 64, 64, D)).reshape(TOKENS, D)
    noise = jax.random.normal(jax.random.fold_in(base_key, 1), (TOKENS, D), jnp.float32)
    value = noise + 0.8 * shared
    return jnp.clip(value, -8.0, 8.0).astype(jnp.bfloat16)


def draw_head_bias(key, part):
    base_key = jax.random.fold_in(key, 23)
    heads = D // HEAD_DIM
    share = 0.5
    decay_low_end = -12.0
    decay_high_end = -10.0
    rate_low_end = -9.0
    rate_high_end = -7.0
    slow_heads = jax.random.bernoulli(jax.random.fold_in(base_key, 1), share, (heads,))
    slow = jnp.repeat(slow_heads, HEAD_DIM)
    decay_fast = jax.random.uniform(jax.random.fold_in(base_key, 2), (D,), jnp.float32, minval=-4.5, maxval=-2.5)
    decay_slow = jax.random.uniform(jax.random.fold_in(base_key, 3), (D,), jnp.float32, minval=decay_low_end, maxval=decay_high_end)
    rate_fast = jax.random.uniform(jax.random.fold_in(base_key, 4), (D,), jnp.float32, minval=-1.0, maxval=1.0)
    rate_slow = jax.random.uniform(jax.random.fold_in(base_key, 5), (D,), jnp.float32, minval=rate_low_end, maxval=rate_high_end)
    decay_row = jnp.where(slow, decay_slow, decay_fast)
    rate_row = jnp.where(slow, rate_slow, rate_fast)
    return jnp.stack([decay_row, rate_row]).astype(jnp.float32)


def levels(stream_key, extent, pieces, low, largest):
    factor_of, own = 1.0, jax.random.fold_in(stream_key, 6)
    for axis_at, blocks in pieces:
        heights = jnp.exp(jax.random.uniform(jax.random.fold_in(own, axis_at), (blocks,), jnp.float32, low / len(pieces), largest / len(pieces)))
        factor_of = factor_of * jnp.repeat(heights, extent[axis_at] // blocks).reshape([-1 if axis == axis_at else 1 for axis in range(len(extent))])
    return factor_of


def centred(own_key, dims, scale, most, pieces=(), dtype=jnp.bfloat16):
    level = levels(own_key, dims, pieces, -0.22, 0.18) if pieces else 1.0
    values = jax.random.normal(own_key, dims, jnp.float32) * scale * level
    return jnp.minimum(jnp.maximum(values, -most), most).astype(dtype)


def setup_inputs(seed: int = 0) -> dict:
    arg_keys = jax.random.split(jax.random.key(seed), 20)
    return {
        "latent": draw_latent(jax.random.fold_in(arg_keys[19], 71), 0),
        "context": centred(arg_keys[1], (CONTEXT, D), 1.0, 6.0, ((0, 8),)),
        "condition": centred(arg_keys[2], (D,), 1.5, 6.0, ((0, 8),), jnp.float32),
        "context_condition": centred(arg_keys[3], (D,), 1.5, 6.0, ((0, 8),), jnp.float32),
        "shift_weight": centred(arg_keys[4], (D, D), D ** -0.5, 0.09375, ((0, 8), (1, 4))),
        "scale_weight": centred(arg_keys[5], (D, D), D ** -0.5, 0.09375, ((0, 8), (1, 4))),
        "gate_weight": centred(arg_keys[6], (D, D), D ** -0.5, 0.09375, ((0, 8), (1, 4))),
        "norm_gain": jnp.clip(1.0 + 0.18 * jax.random.normal(arg_keys[7], (D,), jnp.float32), 0.1, 1.9),
        "decay_down": centred(arg_keys[8], (D, RANK), D ** -0.5, 0.09375),
        "decay_up": centred(arg_keys[9], (RANK, D), RANK ** -0.5, 0.5, ((1, 4),)),
        "rate_down": centred(arg_keys[10], (D, RANK), D ** -0.5, 0.09375),
        "rate_up": centred(arg_keys[11], (RANK, D), RANK ** -0.5, 0.5, ((1, 4),)),
        "head_bias": draw_head_bias(jax.random.fold_in(arg_keys[19], 71), 0),
        "query_weight": centred(arg_keys[13], (D, D), D ** -0.5, 0.09375, ((1, 4),)),
        "key_weight": centred(arg_keys[14], (D, D), D ** -0.5, 0.09375, ((1, 4),)),
        "value_weight": centred(arg_keys[15], (D, D), D ** -0.5, 0.09375, ((1, 4),)),
        "branch_weight": centred(arg_keys[16], (D, D), D ** -0.5, 0.09375, ((1, 4),)),
        "group_gain": jnp.clip(1.0 + 0.18 * jax.random.normal(arg_keys[17], (D,), jnp.float32), 0.1, 1.9),
        "out_weight": centred(arg_keys[18], (D, D), D ** -0.5, 0.09375, ((0, 4),)),
    }


NORM_EPS = 1e-06
GROUP_EPS = 0.00064
DECAY_TOP = math.exp(-0.5)
highest = lax.Precision.HIGHEST

def modulated(rows, gain, scale, shift):
    values = rows.astype(jnp.float32)
    inverse = lax.rsqrt(lax.optimization_barrier(jnp.mean(values * values, axis=-1, keepdims=True)) + NORM_EPS)
    return (values * inverse * gain * (1.0 + scale) + shift).astype(jnp.bfloat16)

def features(normed, key_weight, value_weight, decay_down, decay_up, rate_down, rate_up):
    keys = jnp.dot(normed, key_weight, preferred_element_type=jnp.float32).astype(jnp.bfloat16)
    values = jnp.dot(normed, value_weight, preferred_element_type=jnp.float32).astype(jnp.bfloat16)
    decay_low = jnp.tanh(jnp.dot(normed, decay_down, preferred_element_type=jnp.float32)).astype(jnp.bfloat16)
    rate_low = jnp.dot(normed, rate_down, preferred_element_type=jnp.float32).astype(jnp.bfloat16)
    decay_pre = jnp.dot(decay_low, decay_up, preferred_element_type=jnp.float32).astype(jnp.bfloat16)
    rate_pre = jnp.dot(rate_low, rate_up, preferred_element_type=jnp.float32).astype(jnp.bfloat16)
    return (keys, values, decay_pre, rate_pre)

def chain_inputs(keys, values, decay_pre, rate_pre, head_bias):
    rows = keys.shape[0]
    log_decay = -DECAY_TOP * jax.nn.sigmoid(head_bias[0] + decay_pre.astype(jnp.float32))
    rate = jax.nn.sigmoid(head_bias[1] + rate_pre.astype(jnp.float32))
    key_heads = keys.astype(jnp.float32).reshape(rows, -1, HEAD_DIM)
    unit = key_heads * lax.rsqrt(lax.optimization_barrier(jnp.sum(key_heads * key_heads, axis=-1, keepdims=True)) + 1.0)
    value_heads = values.astype(jnp.float32).reshape(rows, -1, HEAD_DIM)
    write = unit * rate.reshape(rows, -1, HEAD_DIM)
    decay = jnp.exp(log_decay).reshape(rows, -1, HEAD_DIM)
    return (key_heads, value_heads, -unit, write, decay)

def run_chain(state, queries, inputs, reverse):
    key_heads, value_heads, erase, write, decay = inputs

    def advance(carry, item):
        query, key_row, value_row, erase_row, write_row, decay_row = item
        removed = jnp.einsum('hij,hj->hi', carry, erase_row, precision=highest)
        carry = carry * decay_row[:, None, :] + removed[:, :, None] * write_row[:, None, :] + value_row[:, :, None] * key_row[:, None, :]
        return (carry, jnp.einsum('hij,hj->hi', carry, query, precision=highest))
    return lax.scan(advance, state, (queries, key_heads, value_heads, erase, write, decay), reverse=reverse)

def reference(latent, context, condition, context_condition, shift_weight, scale_weight, gate_weight, norm_gain, decay_down, decay_up, rate_down, rate_up, head_bias, query_weight, key_weight, value_weight, branch_weight, group_gain, out_weight):
    conditions = jax.nn.silu(jnp.stack([condition, context_condition])).astype(jnp.bfloat16)
    shift = jnp.dot(conditions, shift_weight, preferred_element_type=jnp.float32)
    scale = jnp.dot(conditions, scale_weight, preferred_element_type=jnp.float32)
    gate = jnp.dot(conditions[:1], gate_weight, preferred_element_type=jnp.float32)[0]
    normed = modulated(latent, norm_gain, scale[0], shift[0])
    normed_context = modulated(context, norm_gain, scale[1], shift[1])
    queries = jnp.dot(normed, query_weight, preferred_element_type=jnp.float32).astype(jnp.bfloat16)
    branch = jnp.dot(normed, branch_weight, preferred_element_type=jnp.float32).astype(jnp.bfloat16)
    latent_in = chain_inputs(*features(normed, key_weight, value_weight, decay_down, decay_up, rate_down, rate_up), head_bias)
    context_in = chain_inputs(*features(normed_context, key_weight, value_weight, decay_down, decay_up, rate_down, rate_up), head_bias)
    query_heads = queries.astype(jnp.float32).reshape(TOKENS, -1, HEAD_DIM)
    zero_state = jnp.zeros((D // HEAD_DIM, HEAD_DIM, HEAD_DIM), jnp.float32)
    reads = jnp.zeros((TOKENS, D // HEAD_DIM, HEAD_DIM), jnp.float32)
    for reverse in (False, True):
        carried, _ = run_chain(zero_state, context_in[0], context_in, reverse)
        _, latent_read = run_chain(carried, query_heads, latent_in, reverse)
        reads = reads + latent_read
    center = lax.optimization_barrier(jnp.mean(reads, axis=-1, keepdims=True))
    variance = lax.optimization_barrier(jnp.mean(jnp.square(reads - center), axis=-1, keepdims=True))
    normal_heads = ((reads - center) * lax.rsqrt(variance + GROUP_EPS)).reshape(TOKENS, D)
    mixed = (normal_heads * group_gain * jax.nn.silu(branch.astype(jnp.float32))).astype(jnp.bfloat16)
    width = D // N_TP
    summed = jnp.zeros((TOKENS, D), jnp.float32)
    for group in range(N_TP):
        partial_sum = jnp.dot(mixed[:, group * width:(group + 1) * width], out_weight[group * width:(group + 1) * width], preferred_element_type=jnp.float32)
        summed = summed + lax.optimization_barrier(partial_sum.astype(jnp.bfloat16)).astype(jnp.float32)
    mixer = summed.astype(jnp.bfloat16).astype(jnp.float32)
    normed_out = mixer * lax.rsqrt(lax.optimization_barrier(jnp.mean(mixer * mixer, axis=-1, keepdims=True)) + NORM_EPS)
    return (latent.astype(jnp.float32) + gate * normed_out).astype(jnp.bfloat16)
```

```python
import functools
import math

import jax
import jax.numpy as jnp
from jax import lax
from jax.experimental import pallas as pl
from jax.experimental.pallas import tpu as pltpu
from jax.sharding import PartitionSpec as P

HEAD_DIM = 64
NORM_EPS = 1e-06
GROUP_EPS = 0.00064
DECAY_TOP = math.exp(-0.5)
BLOCK = 64
F32, BF16 = jnp.float32, jnp.bfloat16


def dot_dims(a, b, left, right):
    return lax.dot_general(
        a.astype(BF16), b.astype(BF16), (((left,), (right,)), ((), ())), preferred_element_type=F32
    )


def mm(a, b):
    return dot_dims(a, b, 1, 0)


def mmt(a, b):
    return dot_dims(a, b, 1, 1)


def tmm(a, b):
    return dot_dims(a, b, 0, 0)


def parts_of(x, count):
    found = []
    for _ in range(count):
        part = x.astype(BF16)
        found.append(part)
        x = x - part.astype(F32)
    return found


def head_ones(width):
    row = lax.broadcasted_iota(jnp.int32, (width, width), 0) // HEAD_DIM
    col = lax.broadcasted_iota(jnp.int32, (width, width), 1) // HEAD_DIM
    return (row == col).astype(F32)


def group_sum(x, ones, count=3):
    return sum(mm(part, ones) for part in parts_of(x, count))


def stack_heads(x):
    x = x.astype(BF16)
    count = x.shape[1] // HEAD_DIM
    if count == 1:
        return x
    lane = lax.broadcasted_iota(jnp.int32, (1, x.shape[1]), 1) // HEAD_DIM
    return jnp.concatenate([x * (lane == h).astype(F32).astype(BF16) for h in range(count)], axis=0)


def pack_heads(x):
    return sum(x[at : at + HEAD_DIM] for at in range(0, x.shape[0], HEAD_DIM))


def chain_inputs(keys, decay_pre, rate_pre, head_bias):
    k = keys.astype(F32)
    log_decay = -DECAY_TOP * jax.nn.sigmoid(head_bias[0:1] + decay_pre.astype(F32))
    rate = jax.nn.sigmoid(head_bias[1:2] + rate_pre.astype(F32))
    unit = k * lax.rsqrt(group_sum(k * k, head_ones(k.shape[1]), 2) + 1.0)
    return k, -unit, unit * rate, log_decay


def cumulate(log_decay, sign):
    row = lax.broadcasted_iota(jnp.int32, (BLOCK, BLOCK), 0)
    col = lax.broadcasted_iota(jnp.int32, (BLOCK, BLOCK), 1)
    mask = ((row - col) * sign >= 0).astype(F32)
    return sum(mm(mask, part) for part in parts_of(log_decay, 3))


def solve_blocks(items, width):
    row = lax.broadcasted_iota(jnp.int32, (BLOCK, width), 0)
    col = lax.broadcasted_iota(jnp.int32, (BLOCK, width), 1) % BLOCK
    ones = head_ones(width)
    square = lax.broadcasted_iota(jnp.int32, (width, width), 0)
    unit = (square == lax.broadcasted_iota(jnp.int32, (width, width), 1)).astype(F32)
    one = (row == col).astype(F32)
    work = []
    for sign, k, v, erase, write, log_decay, cum, q in items:
        strict = (row - col) * sign > 0
        inclusive = (row - col) * sign >= 0
        growth = jnp.exp(-cum)
        es = (erase * jnp.exp(cum - log_decay)).astype(BF16)
        right_w, right_k = stack_heads(write * growth), stack_heads(k * growth)
        item = {"es": es, "v": v.astype(BF16)}
        if q is not None:
            qs = q * jnp.exp(cum)
            left = jnp.concatenate([es, qs.astype(BF16)], axis=0)
        else:
            left = es
        by_w, by_k = mmt(left, right_w), mmt(left, right_k)
        item["coupling"] = jnp.where(strict, by_w[:BLOCK], 0.0)
        item["feed"] = jnp.where(strict, by_k[:BLOCK], 0.0)
        if q is not None:
            item["qs"] = qs
            item["aw"] = jnp.where(inclusive, by_w[BLOCK:], 0.0)
            item["ak"] = jnp.where(inclusive, by_k[BLOCK:], 0.0)
        if isinstance(sign, int):
            final = cum[BLOCK - 1 :] if sign > 0 else cum[0:1]
        else:
            final = jnp.where(sign > 0, cum[BLOCK - 1 :], cum[0:1])
        tail = jnp.exp(final - cum)
        item["wt"], item["kt"] = (write * tail).astype(BF16), (k * tail).astype(BF16)
        item["diagonal"] = unit * jnp.exp(final)
        work.append(item)
    near = (row // 2 == col // 2) & (row != col)
    for item in work:
        item["x"] = one + jnp.where(near, item["coupling"], 0.0)
        seen = stack_heads(item["v"])
        if "ak" in item:
            both = mm(jnp.concatenate([item["feed"], item["ak"]], axis=0), seen)
            item["fed"], item["akv"] = both[:BLOCK], both[BLOCK:]
        else:
            item["fed"] = mm(item["feed"], seen)
    size = 2
    while size < BLOCK:
        level = (row // (2 * size) == col // (2 * size)) & (row // size != col // size)
        for item in work:
            item["y"] = mm(jnp.where(level, item["coupling"], 0.0), stack_heads(item["x"]))
        for item in work:
            item["x"] = item["x"] + mm(item["x"], stack_heads(item["y"]))
        size *= 2
    for item in work:
        item["response"] = mm(item["x"], stack_heads(item["es"]))
        item["offset"] = mm(item["x"], stack_heads(item["fed"]))
    done = []
    for item in work:
        transfer = tmm(item["response"], item["wt"]) * ones + item["diagonal"]
        constant = (tmm(item["offset"], item["wt"]) + tmm(item["v"], item["kt"])) * ones
        if "aw" in item:
            query = item["qs"] + mm(item["aw"], stack_heads(item["response"]))
            base = item["akv"] + mm(item["aw"], stack_heads(item["offset"]))
            done.append((transfer, constant, query, base))
        else:
            done.append((transfer, constant, None, None))
    return done


MESH = pl.DeviceIdType.MESH


def solve_pack(k, v, erase, write, log_decay, q, signs):
    items = []
    for sign in signs:
        for at in range(0, k.shape[0], BLOCK):
            r = slice(at, at + BLOCK)
            cum = cumulate(log_decay[r], sign)
            items.append(
                (sign, k[r], v[r], erase[r], write[r], log_decay[r], cum, None if q is None else q[r])
            )
    return items


def advance(state, transfer, constant):
    high, low = parts_of(state, 2)
    both = mm(jnp.concatenate([high, low], axis=0), transfer)
    return both[:HEAD_DIM] + both[HEAD_DIM:] + constant


class Plan:
    def __init__(self, sp, tp, rows, context_rows, depth, local):
        self.sp, self.tp, self.chips = sp, tp, tp // 2
        self.block, self.context_rows = rows, context_rows
        self.rows = rows * tp
        self.depth, self.local = depth, local
        heads = local // HEAD_DIM
        self.width = (2 if heads % sp == 0 else 1) * HEAD_DIM
        self.packs = local // self.width
        self.units = 2 * self.packs // sp
        assert self.units in (1, 2) and self.units * sp == 2 * self.packs
        self.chunk = max(128, local // sp)
        self.owners = local // self.chunk
        self.tile = 512
        self.out_tile = 1024
        self.out_tiles = depth // self.out_tile
        self.context_blocks = context_rows * sp // BLOCK


def remote(source, target, sent, taken, **peer):
    return pltpu.make_async_remote_copy(
        src_ref=source,
        dst_ref=target,
        send_sem=sent,
        recv_sem=taken,
        device_id=peer,
        device_id_type=MESH,
    )


def layer_kernel(
    plan,
    latent_hbm, context_hbm, condition_ref, context_condition_ref,
    shift_hbm, scale_hbm, gate_hbm, norm_gain_ref,
    decay_down_hbm, decay_up_hbm, rate_down_hbm, rate_up_hbm, bias_ref,
    query_hbm, key_hbm, value_hbm, branch_hbm, group_gain_ref, out_hbm,
    updated_ref,
    rows_v, context_v, wmod_v, wdown_v, wup_v, wbig_v, wout_v,
    parts_v, part_in_v, vectors_v, mod_v, gate_v, inverse_v, normed_v,
    key_v, value_v, decay_v, rate_v, query_v, branch_v, bias_v,
    feature_out_v, feature_in_v, maps_out_v, maps_in_v, reads_q_v, base_v,
    transfer_v, constant_v, entry_out_v, entry_in_v, mixed_v,
    partial_v, pair_v, cross_out_v, cross_in_v, mixer_v,
    local_sem, row_s, row_r, relay_s, relay_r, part_s, part_r, vec_s, vec_r,
    feat_s, feat_r, map_s, map_r, ent_s, ent_r, pair_s, pair_r, cross_s, cross_r,
):
    sp, tp, chips, width, packs, units = plan.sp, plan.tp, plan.chips, plan.width, plan.packs, plan.units
    depth, local, block = plan.depth, plan.local, plan.block
    me_sp, me_tp = lax.axis_index("sp"), lax.axis_index("tp")
    chip, core = me_tp // 2, lax.rem(me_tp, 2)
    sibling = chip * 2 + 1 - core

    fetches = {}

    def fetch(name, at, source, target):
        copy = pltpu.make_async_copy(source, target, local_sem.at[at])
        copy.start()
        fetches[name] = copy

    fetch("shift", 0, shift_hbm, wmod_v.at[0])
    fetch("scale", 1, scale_hbm, wmod_v.at[1])
    fetch("gate", 2, gate_hbm, wmod_v.at[2])
    fetch("latent", 3, latent_hbm, rows_v.at[me_tp])
    fetch("context", 4, context_hbm, context_v)

    barrier = pltpu.get_barrier_semaphore()
    everyone = [(a, b) for a in range(sp) for b in range(tp) if (a, b) != (0, 0)]
    for a, b in everyone:
        pl.semaphore_signal(
            barrier,
            inc=1,
            device_id={"sp": lax.rem(me_sp + a, sp), "tp": lax.rem(me_tp + b, tp)},
            device_id_type=MESH,
        )

    fetch("decay_down", 5, decay_down_hbm, wdown_v.at[:, 0 : decay_down_hbm.shape[1]])
    fetch("rate_down", 6, rate_down_hbm, wdown_v.at[:, decay_down_hbm.shape[1] :])
    line = lax.broadcasted_iota(jnp.int32, (8, condition_ref.shape[1]), 0)
    values = jnp.where(line == 0, condition_ref[...], jnp.where(line == 1, context_condition_ref[...], 0.0))
    conditions = (values * jax.nn.sigmoid(values)).astype(BF16)
    shares = []
    for at, name in enumerate(("shift", "scale", "gate")):
        fetches[name].wait()
        shares.append(mm(conditions, wmod_v[at])[0:2])
    fetch("key", 7, key_hbm, wbig_v.at[0])
    fetch("value", 8, value_hbm, wbig_v.at[1])
    shares = jnp.concatenate(shares + [jnp.zeros_like(shares[0])], axis=0)
    for j in range(plan.owners):
        parts_v[j] = shares[:, j * plan.chunk : (j + 1) * plan.chunk]

    pl.semaphore_wait(barrier, len(everyone))

    def part_copy(d):
        peer = lax.rem(me_sp + d, sp)
        return peer, remote(
            parts_v.at[peer], part_in_v.at[d - 1], part_s.at[d - 1], part_r.at[d - 1], sp=peer, tp=me_tp
        )

    def when_owner(at, body):
        if plan.owners == sp:
            body()
        else:
            pl.when(at < plan.owners)(body)

    for d in range(1, sp):
        peer = lax.rem(me_sp + d, sp)
        when_owner(peer, lambda d=d: part_copy(d)[1].start())

    fetches["latent"].wait()

    def slot_of(d, c):
        return lax.rem(chip - d + chips, chips) * 2 + c

    row_copies = [
        remote(
            rows_v.at[me_tp], rows_v.at[me_tp], row_s.at[d - 1], row_r.at[d - 1],
            sp=me_sp, tp=lax.rem(chip + d, chips) * 2 + core,
        )
        for d in range(1, chips)
    ]
    relay_copies = [
        remote(
            rows_v.at[slot_of(d, core)], rows_v.at[slot_of(d, core)], relay_s.at[d], relay_r.at[d],
            sp=me_sp, tp=sibling,
        )
        for d in range(chips)
    ]
    relay_arrivals = [
        remote(
            rows_v.at[slot_of(d, 1 - core)], rows_v.at[slot_of(d, 1 - core)], relay_s.at[d], relay_r.at[d],
            sp=me_sp, tp=sibling,
        )
        for d in range(chips)
    ]
    row_arrivals = [
        remote(
            rows_v.at[slot_of(d, core)], rows_v.at[slot_of(d, core)], row_s.at[d - 1], row_r.at[d - 1],
            sp=me_sp, tp=lax.rem(chip + d, chips) * 2 + core,
        )
        for d in range(1, chips)
    ]
    for copy in row_copies:
        copy.start()
    relay_copies[0].start()

    my_slot = me_tp * plan.owners + me_sp
    vector_copies = [
        remote(
            vectors_v.at[my_slot], vectors_v.at[my_slot], vec_s.at[a * tp + b], vec_r.at[a * tp + b],
            sp=lax.rem(me_sp + a, sp), tp=lax.rem(me_tp + b, tp),
        )
        for a, b in everyone
    ]

    def own_columns():
        total = parts_v[me_sp]
        for d in range(1, sp):
            part_copy(d)[1].wait_recv()
            total = total + part_in_v[d - 1]
        vectors_v[my_slot] = total
        for copy in vector_copies:
            copy.start()

    when_owner(me_sp, own_columns)

    fetch("decay_up", 9, decay_up_hbm, wup_v.at[0])
    fetch("rate_up", 10, rate_up_hbm, wup_v.at[1])
    fetch("query", 11, query_hbm, wbig_v.at[2])
    fetch("branch", 12, branch_hbm, wbig_v.at[3])

    def inverse_of(x):
        x = x.astype(F32)
        mean = jnp.sum(x * x, axis=-1, keepdims=True) * (1.0 / depth)
        return jnp.broadcast_to(lax.rsqrt(mean + NORM_EPS), (16, 128))

    fetches["context"].wait()
    for at in range(0, plan.context_rows, 16):
        inverse_v[(plan.rows + at) // 16] = inverse_of(context_v[at : at + 16])

    def block_inverse(slot):
        for at in range(0, block, 16):
            inverse_v[(slot * block + at) // 16] = inverse_of(rows_v[slot, at : at + 16])

    block_inverse(me_tp)
    relay_arrivals[0].wait_recv()
    block_inverse(sibling)
    for d in range(1, chips):
        row_arrivals[d - 1].wait_recv()
        relay_copies[d].start()
        block_inverse(slot_of(d, core))
    for d in range(1, chips):
        relay_arrivals[d].wait_recv()
        block_inverse(slot_of(d, 1 - core))
    for p in range(packs):
        bias_v[p] = bias_ref[:, p * width : (p + 1) * width]

    for a, b in everyone:
        from_sp, from_tp = lax.rem(me_sp - a + sp, sp), lax.rem(me_tp - b + tp, tp)
        slot = from_tp * plan.owners + from_sp

        def take(a=a, b=b, slot=slot):
            remote(
                vectors_v.at[slot], vectors_v.at[slot], vec_s.at[a * tp + b], vec_r.at[a * tp + b],
                sp=me_sp, tp=me_tp,
            ).wait_recv()

        when_owner(from_sp, take)

    for j in range(tp * plan.owners):
        c = slice(j * plan.chunk, (j + 1) * plan.chunk)
        tile = vectors_v[j]
        mod_v[0:2, c] = norm_gain_ref[:, c] * (1.0 + tile[2:4])
        mod_v[2:4, c] = tile[0:2]
        gate_v[:, c] = tile[4:5]

    def modulate(read, group, which):
        inverse = inverse_v[group][:, 0:1]
        for at in range(0, depth, 512):
            c = slice(at, at + 512)
            x = read(c).astype(F32) * inverse * mod_v[which : which + 1, c] + mod_v[2 + which : 3 + which, c]
            normed_v[pl.ds(pl.multiple_of(group * 16, 16), 16), c] = x.astype(BF16)

    per = block // 16

    @pl.loop(0, plan.rows // 16)
    def _(g):
        slot, at = g // per, lax.rem(g, per) * 16
        modulate(lambda c: rows_v[slot, pl.ds(pl.multiple_of(at, 16), 16), c], g, 0)

    for at in range(0, plan.context_rows, 16):
        modulate(lambda c: context_v[at : at + 16, c], (plan.rows + at) // 16, 1)

    fetch("out", 13, out_hbm, wout_v)

    rank = decay_down_hbm.shape[1]
    fetches["decay_down"].wait()
    fetches["rate_down"].wait()
    low = jnp.dot(normed_v[...], wdown_v[...], preferred_element_type=F32)
    decay_low = jnp.tanh(low[:, :rank]).astype(BF16)
    rate_low = low[:, rank:].astype(BF16)

    def spread(found, at, target, kind):
        found = found.astype(BF16)
        for p in range(found.shape[1] // width):
            piece = found[:, p * width : (p + 1) * width]
            target[at // width + p] = piece[: plan.rows]
            if kind is not None:
                feature_out_v[at // width + p, kind] = piece[plan.rows :]

    for name, lhs, which, target, kind in (
        ("decay_up", decay_low, 0, decay_v, 2),
        ("rate_up", rate_low, 1, rate_v, 3),
    ):
        fetches[name].wait()
        for at in range(0, local, plan.tile):
            found = jnp.dot(lhs, wup_v[which, :, at : at + plan.tile], preferred_element_type=F32)
            spread(found, at, target, kind)

    def project(name, which, rows, target, kind):
        fetches[name].wait()
        for at in range(0, local, plan.tile):
            found = jnp.dot(
                normed_v[0:rows], wbig_v[which, :, at : at + plan.tile], preferred_element_type=F32
            )
            spread(found, at, target, kind)

    everything = plan.rows + plan.context_rows
    project("key", 0, everything, key_v, 0)
    project("value", 1, everything, value_v, 1)

    def pack_of(d):
        return (d * units) // 2

    def feature_copy(d):
        peer = lax.rem(me_sp + d, sp)
        return remote(
            feature_out_v.at[pack_of(peer)], feature_in_v.at[me_sp], feat_s.at[d - 1], feat_r.at[d - 1],
            sp=peer, tp=me_tp,
        )

    for d in range(1, sp):
        feature_copy(d).start()
    feature_in_v[me_sp] = feature_out_v[pack_of(me_sp)]

    project("query", 2, plan.rows, query_v, None)

    def maps_copy(d):
        peer = lax.rem(me_sp + d, sp)
        return remote(
            maps_out_v.at[pl.ds(peer * units, units)], maps_in_v.at[me_sp], map_s.at[d - 1], map_r.at[d - 1],
            sp=peer, tp=me_tp,
        )

    blocks = plan.rows // BLOCK
    group = min(2, packs)
    first = pack_of(me_sp)

    @pl.loop(0, packs // group)
    def _(s):
        at = [lax.rem(first + 1 + s * group + i, packs) for i in range(group)]
        items = []
        for p in at:
            k, erase, write, log_decay = chain_inputs(key_v[p], decay_v[p], rate_v[p], bias_v[p])
            items += solve_pack(k, value_v[p], erase, write, log_decay, query_v[p].astype(F32), (1, -1))
        found = solve_blocks(items, width)
        for i, p in enumerate(at):
            bases = [None] * blocks
            for way in (0, 1):
                mine = found[(i * 2 + way) * blocks : (i * 2 + way + 1) * blocks]
                carried = None
                for b in range(blocks) if way == 0 else reversed(range(blocks)):
                    transfer, constant, query, base = mine[b]
                    if carried is not None:
                        base = base + mmt(query, carried[1])
                        query = mmt(query, carried[0])
                        transfer, constant = (
                            mm(carried[0], transfer),
                            mm(carried[1], transfer) + constant,
                        )
                    carried = (transfer, constant)
                    reads_q_v[p, way, b * BLOCK : (b + 1) * BLOCK] = query.astype(BF16)
                    bases[b] = base if bases[b] is None else bases[b] + base
                maps_out_v[p * 2 + way, 0] = pack_heads(carried[0]).astype(BF16)
                maps_out_v[p * 2 + way, 1] = pack_heads(carried[1]).astype(BF16)
            for b in range(blocks):
                base_v[p, b * BLOCK : (b + 1) * BLOCK] = bases[b]
            if units == 2:
                d = 1 + s * group + i

                @pl.when(d < sp)
                def _():
                    maps_copy(d).start()

    if units == 1:
        for d in range(1, sp):
            maps_copy(d).start()
    maps_in_v[me_sp] = maps_out_v[pl.ds(me_sp * units, units)]

    for d in range(1, sp):
        source = lax.rem(me_sp - d + sp, sp)
        remote(
            feature_out_v.at[0], feature_in_v.at[source], feat_s.at[d - 1], feat_r.at[d - 1],
            sp=me_sp, tp=me_tp,
        ).wait_recv()
    keys, vals, decay_pre, rate_pre = (
        jnp.concatenate([feature_in_v[at, kind] for at in range(sp)], axis=0) for kind in range(4)
    )
    k, erase, write, log_decay = chain_inputs(keys, decay_pre, rate_pre, bias_v[first])
    count = plan.context_blocks
    if units == 2:
        signs, ways = (1, -1), (0, 1)
    else:
        ways = (lax.rem(me_sp, 2),)
        signs = (1 - 2 * ways[0],)
    found = solve_blocks(solve_pack(k, vals, erase, write, log_decay, None, signs), width)
    states = []
    for u in range(units):
        mine = found[u * count : (u + 1) * count]
        if units == 2:
            order = mine if u == 0 else mine[::-1]
            state = order[0][1]
            state = pack_heads(state)
            for transfer, constant, _, _ in order[1:]:
                state = advance(state, transfer, pack_heads(constant))
        else:
            for b, (transfer, constant, _, _) in enumerate(mine):
                transfer_v[b] = transfer.astype(BF16)
                constant_v[b] = pack_heads(constant)
            state = constant_v[jnp.where(ways[0] == 1, count - 1, 0)]
            for step in range(1, count):
                b = jnp.where(ways[0] == 1, count - 1 - step, step)
                state = advance(state, transfer_v[b], constant_v[b])
        states.append(state)

    project("branch", 3, plan.rows, branch_v, None)

    for d in range(1, sp):
        source = lax.rem(me_sp - d + sp, sp)
        remote(
            maps_out_v.at[pl.ds(0, units)], maps_in_v.at[source], map_s.at[d - 1], map_r.at[d - 1],
            sp=me_sp, tp=me_tp,
        ).wait_recv()

    def entry_copy(u, at):
        return remote(
            entry_out_v.at[at, u], entry_in_v.at[me_sp * units + u],
            ent_s.at[u, lax.rem(at - me_sp + sp, sp)], ent_r.at[u, lax.rem(at - me_sp + sp, sp)],
            sp=at, tp=me_tp,
        )

    for step in range(sp):
        for u in range(units):
            if units == 2:
                at = step if u == 0 else sp - 1 - step
            else:
                at = jnp.where(ways[0] == 1, sp - 1 - step, step)
            entry_out_v[at, u] = states[u].astype(BF16)

            @pl.when(at != me_sp)
            def _(u=u, at=at):
                entry_copy(u, at).start()

        if step < sp - 1:
            for u in range(units):
                if units == 2:
                    at = step if u == 0 else sp - 1 - step
                else:
                    at = jnp.where(ways[0] == 1, sp - 1 - step, step)
                states[u] = advance(
                    states[u], stack_heads(maps_in_v[at, u, 0]), maps_in_v[at, u, 1].astype(F32)
                )
    for u in range(units):
        entry_in_v[me_sp * units + u] = entry_out_v[me_sp, u]

    for d in range(1, sp):
        source = lax.rem(me_sp - d + sp, sp)
        for u in range(units):
            remote(
                entry_out_v.at[0, u], entry_in_v.at[source * units + u], ent_s.at[u, d], ent_r.at[u, d],
                sp=me_sp, tp=me_tp,
            ).wait_recv()

    ones = head_ones(width)
    for p in range(packs):
        c = slice(p * width, (p + 1) * width)
        reads = base_v[p]
        for way in (0, 1):
            reads = reads + mmt(reads_q_v[p, way], stack_heads(entry_in_v[2 * p + way]))
        away = reads - group_sum(reads, ones) * (1.0 / HEAD_DIM)
        variance = group_sum(away * away, ones) * (1.0 / HEAD_DIM)
        gates = branch_v[p].astype(F32)
        mixed_v[:, c] = (
            away * lax.rsqrt(variance + GROUP_EPS) * group_gain_ref[:, c] * (gates * jax.nn.sigmoid(gates))
        ).astype(BF16)

    fetches["out"].wait()

    def pair_copy(j):
        return remote(
            partial_v.at[j, 1 - core], pair_v.at[j], pair_s.at[j], pair_r.at[j], sp=me_sp, tp=sibling
        )

    def cross_copy(j, d):
        return remote(
            cross_out_v.at[j, d - 1], cross_in_v.at[j, d - 1], cross_s.at[j, d - 1], cross_r.at[j, d - 1],
            sp=me_sp, tp=lax.rem(chip + d, chips) * 2 + core,
        )

    for j in range(plan.out_tiles + 1):
        if j < plan.out_tiles:
            c = slice(j * plan.out_tile, (j + 1) * plan.out_tile)
            found = mm(mixed_v[...], wout_v[:, c]).astype(BF16)
            for t in range(tp):
                partial_v[j, t % 2, t // 2] = found[t * block : (t + 1) * block]
            pair_copy(j).start()
        if j > 0:
            i = j - 1
            pair_copy(i).wait_recv()
            for d in range(1, chips):
                to = lax.rem(chip + d, chips)
                cross_out_v[i, d - 1] = (
                    partial_v[i, core, to].astype(F32) + pair_v[i, to].astype(F32)
                ).astype(BF16)
                cross_copy(i, d).start()
    square = jnp.zeros((block, 1), F32)
    for j in range(plan.out_tiles):
        c = slice(j * plan.out_tile, (j + 1) * plan.out_tile)
        total = partial_v[j, core, chip].astype(F32) + pair_v[j, chip].astype(F32)
        for d in range(1, chips):
            cross_copy(j, d).wait_recv()
            total = total + cross_in_v[j, d - 1].astype(F32)
        total = total.astype(BF16).astype(F32)
        mixer_v[:, c] = total
        square = square + jnp.sum(total * total, axis=-1, keepdims=True)
    inverse = lax.rsqrt(square * (1.0 / depth) + NORM_EPS)
    for at in range(0, depth, 512):
        c = slice(at, at + 512)
        updated_ref[:, c] = (
            rows_v[me_tp, :, c].astype(F32) + gate_v[:, c] * (mixer_v[:, c] * inverse)
        ).astype(BF16)

    for d in range(1, sp):
        when_owner(lax.rem(me_sp + d, sp), lambda d=d: part_copy(d)[1].wait_send())
    for copy in row_copies + relay_copies:
        copy.wait_send()

    def vectors_left():
        for copy in vector_copies:
            copy.wait_send()

    when_owner(me_sp, vectors_left)
    for d in range(1, sp):
        feature_copy(d).wait_send()
        maps_copy(d).wait_send()
        for u in range(units):
            entry_copy(u, lax.rem(me_sp + d, sp)).wait_send()
    for j in range(plan.out_tiles):
        pair_copy(j).wait_send()
        for d in range(1, chips):
            cross_copy(j, d).wait_send()


def on_device(
    latent,
    context,
    condition,
    context_condition,
    shift_weight,
    scale_weight,
    gate_weight,
    norm_gain,
    decay_down,
    decay_up,
    rate_down,
    rate_up,
    head_bias,
    query_weight,
    key_weight,
    value_weight,
    branch_weight,
    group_gain,
    out_weight,
):
    sp, tp = lax.axis_size("sp"), lax.axis_size("tp")
    block, depth = latent.shape
    local = query_weight.shape[1]
    plan = Plan(sp, tp, block, context.shape[0], depth, local)
    width, packs, units, chips = plan.width, plan.packs, plan.units, plan.chips
    rows, crows, tiles = plan.rows, plan.context_rows, plan.out_tiles
    rank = decay_down.shape[1]
    vmem = pl.BlockSpec(memory_space=pltpu.VMEM)
    hbm = pl.BlockSpec(memory_space=pltpu.HBM)
    scratch = [
        ((tp, block, depth), BF16),
        ((crows, depth), BF16),
        ((3, *shift_weight.shape), BF16),
        ((depth, 2 * rank), BF16),
        ((2, rank, local), BF16),
        ((4, depth, local), BF16),
        ((local, depth), BF16),
        ((plan.owners, 8, plan.chunk), F32),
        ((sp - 1, 8, plan.chunk), F32),
        ((tp * plan.owners, 8, plan.chunk), F32),
        ((8, depth), F32),
        ((1, depth), F32),
        (((rows + crows) // 16, 16, 128), F32),
        ((rows + crows, depth), BF16),
        ((packs, rows, width), BF16),
        ((packs, rows, width), BF16),
        ((packs, rows, width), BF16),
        ((packs, rows, width), BF16),
        ((packs, rows, width), BF16),
        ((packs, rows, width), BF16),
        ((packs, 2, width), F32),
        ((packs, 4, crows, width), BF16),
        ((sp, 4, crows, width), BF16),
        ((2 * packs, 2, HEAD_DIM, width), BF16),
        ((sp, units, 2, HEAD_DIM, width), BF16),
        ((packs, 2, rows, width), BF16),
        ((packs, rows, width), F32),
        ((plan.context_blocks, width, width), BF16),
        ((plan.context_blocks, HEAD_DIM, width), F32),
        ((sp, units, HEAD_DIM, width), BF16),
        ((2 * packs, HEAD_DIM, width), BF16),
        ((rows, local), BF16),
        ((tiles, 2, chips, block, plan.out_tile), BF16),
        ((tiles, chips, block, plan.out_tile), BF16),
        ((tiles, chips - 1, block, plan.out_tile), BF16),
        ((tiles, chips - 1, block, plan.out_tile), BF16),
        ((block, depth), F32),
    ]
    semaphores = [
        (14,),
        (chips - 1,), (chips - 1,), (chips,), (chips,), (sp - 1,), (sp - 1,), (sp * tp,), (sp * tp,),
        (sp - 1,), (sp - 1,), (sp - 1,), (sp - 1,), (units, sp), (units, sp),
        (tiles,), (tiles,), (tiles, chips - 1), (tiles, chips - 1),
    ]
    return pl.pallas_call(
        functools.partial(layer_kernel, plan),
        in_specs=[hbm, hbm, vmem, vmem, hbm, hbm, hbm, vmem, hbm, hbm, hbm, hbm, vmem, hbm, hbm, hbm, hbm, vmem, hbm],
        out_specs=vmem,
        out_shape=jax.ShapeDtypeStruct(latent.shape, BF16),
        scratch_shapes=[pltpu.VMEM(shape, kind) for shape, kind in scratch]
        + [pltpu.SemaphoreType.DMA(shape) for shape in semaphores],
        compiler_params=pltpu.CompilerParams(
            collective_id=0, has_side_effects=True, vmem_limit_bytes=67043328
        ),
        name="layer",
    )(
        latent, context, condition.reshape(1, -1), context_condition.reshape(1, -1),
        shift_weight, scale_weight, gate_weight, norm_gain.reshape(1, -1),
        decay_down, decay_up, rate_down, rate_up, head_bias,
        query_weight, key_weight, value_weight, branch_weight, group_gain.reshape(1, -1), out_weight,
    )


def solution(mesh):
    placed = (
        P(("sp", "tp"), None),
        P("sp", None),
        P("sp"),
        P("sp"),
        P("sp", "tp"),
        P("sp", "tp"),
        P("sp", "tp"),
        P(),
        P(),
        P(None, "tp"),
        P(),
        P(None, "tp"),
        P(None, "tp"),
        P(None, "tp"),
        P(None, "tp"),
        P(None, "tp"),
        P(None, "tp"),
        P("tp"),
        P("tp", None),
    )
    return jax.shard_map(
        on_device, mesh=mesh, in_specs=placed, out_specs=P(("sp", "tp"), None), check_vma=False
    )
```

```python
import functools
import math

import jax
import jax.numpy as jnp
from jax import lax
from jax.experimental import pallas as pl
from jax.experimental.pallas import tpu as pltpu
from jax.sharding import PartitionSpec as P

HEAD_DIM = 64
NORM_EPS = 1e-06
GROUP_EPS = 0.00064
DECAY_TOP = math.exp(-0.5)
BLOCK = 64
VMEM_BYTES = 67043328
F32, BF16 = jnp.float32, jnp.bfloat16


def dot_dims(a, b, left, right):
    return lax.dot_general(
        a.astype(BF16), b.astype(BF16), (((left,), (right,)), ((), ())), preferred_element_type=F32
    )


def mm(a, b):
    return dot_dims(a, b, 1, 0)


def mmt(a, b):
    return dot_dims(a, b, 1, 1)


def tmm(a, b):
    return dot_dims(a, b, 0, 0)


def parts_of(x, count):
    found = []
    for _ in range(count):
        part = x.astype(BF16)
        found.append(part)
        x = x - part.astype(F32)
    return found


def head_ones(width):
    row = lax.broadcasted_iota(jnp.int32, (width, width), 0) // HEAD_DIM
    col = lax.broadcasted_iota(jnp.int32, (width, width), 1) // HEAD_DIM
    return (row == col).astype(F32)


def group_sum(x, ones, count=3):
    return sum(mm(part, ones) for part in parts_of(x, count))


def stack_heads(x):
    x = x.astype(BF16)
    count = x.shape[1] // HEAD_DIM
    if count == 1:
        return x
    lane = lax.broadcasted_iota(jnp.int32, (1, x.shape[1]), 1) // HEAD_DIM
    return jnp.concatenate([x * (lane == h).astype(F32).astype(BF16) for h in range(count)], axis=0)


def pack_heads(x):
    return sum(x[at : at + HEAD_DIM] for at in range(0, x.shape[0], HEAD_DIM))


def chain_inputs(keys, decay_pre, rate_pre, head_bias):
    k = keys.astype(F32)
    log_decay = -DECAY_TOP * jax.nn.sigmoid(head_bias[0:1] + decay_pre.astype(F32))
    rate = jax.nn.sigmoid(head_bias[1:2] + rate_pre.astype(F32))
    unit = k * lax.rsqrt(group_sum(k * k, head_ones(k.shape[1]), 2) + 1.0)
    return k, -unit, unit * rate, log_decay


def block_sums(log_decay):
    size = log_decay.shape[0]
    row = lax.broadcasted_iota(jnp.int32, (size, size), 0)
    col = lax.broadcasted_iota(jnp.int32, (size, size), 1)
    mask = ((row >= col) & (row // BLOCK == col // BLOCK)).astype(F32)
    return sum(mm(mask, part) for part in parts_of(log_decay, 3))


def pack_items(k, v, erase, write, log_decay, signs):
    items, ahead = [], block_sums(log_decay)
    for sign in signs:
        for at in range(0, k.shape[0], BLOCK):
            r = slice(at, at + BLOCK)
            total = ahead[at + BLOCK - 1 : at + BLOCK]
            cum = ahead[r]
            if not isinstance(sign, int):
                cum = jnp.where(sign > 0, cum, total - cum + log_decay[r])
            elif sign < 0:
                cum = total - cum + log_decay[r]
            items.append((sign, k[r], v[r], erase[r], write[r], log_decay[r], cum, total))
    return items


def signed_masks(sign, width):
    row = lax.broadcasted_iota(jnp.int32, (BLOCK, width), 0)
    col = lax.broadcasted_iota(jnp.int32, (BLOCK, width), 1) % BLOCK
    return (row - col) * sign > 0, (row - col) * sign >= 0


def beside(left, right):
    return jnp.concatenate([stack_heads(left), stack_heads(right)], axis=1)


def above(left, right):
    return jnp.concatenate([stack_heads(left), stack_heads(right)], axis=0)


def solve_maps(items, width):
    row = lax.broadcasted_iota(jnp.int32, (BLOCK, width), 0)
    col = lax.broadcasted_iota(jnp.int32, (BLOCK, width), 1) % BLOCK
    ones = head_ones(width)
    square = lax.broadcasted_iota(jnp.int32, (width, width), 0)
    unit = (square == lax.broadcasted_iota(jnp.int32, (width, width), 1)).astype(F32)
    one = (row == col).astype(F32)
    near = (row // 2 == col // 2) & (row != col)
    work = []
    for sign, k, v, erase, write, log_decay, cum, total in items:
        strict, _ = signed_masks(sign, width)
        growth = jnp.exp(-cum)
        item = {"es": (erase * jnp.exp(cum - log_decay)).astype(BF16), "v": v.astype(BF16), "cum": cum}
        item["wg"], item["kg"] = (write * growth).astype(BF16), (k * growth).astype(BF16)
        both = mmt(item["es"], above(item["wg"], item["kg"]))
        item["coupling"] = jnp.where(strict, both[:, :width], 0.0)
        item["feed"] = jnp.where(strict, both[:, width:], 0.0)
        tail = jnp.exp(total - cum)
        item["wt"], item["kt"] = (write * tail).astype(BF16), (k * tail).astype(BF16)
        item["diagonal"] = unit * jnp.exp(total)
        work.append(item)
    for item in work:
        item["x"] = one + jnp.where(near, item["coupling"], 0.0)
        item["fed"] = mm(item["feed"], stack_heads(item["v"]))
    size = 2
    while size < BLOCK:
        level = (row // (2 * size) == col // (2 * size)) & (row // size != col // size)
        for item in work:
            item["y"] = mm(jnp.where(level, item["coupling"], 0.0), stack_heads(item["x"]))
        for item in work:
            item["x"] = item["x"] + mm(item["x"], stack_heads(item["y"]))
        size *= 2
    for item in work:
        both = mm(item["x"], beside(item["es"], item["fed"])).astype(BF16)
        item["both"] = both
        item["response"], item["offset"] = both[:, :width], both[:, width:]
    for item in work:
        moved = tmm(item["both"], item["wt"])
        item["transfer"] = moved[:width] * ones + item["diagonal"]
        item["constant"] = (moved[width:] + tmm(item["v"], item["kt"])) * ones
    return work


MESH = pl.DeviceIdType.MESH


def advance(state, transfer, constant):
    high, low = parts_of(state, 2)
    both = mm(jnp.concatenate([high, low], axis=0), transfer)
    return both[:HEAD_DIM] + both[HEAD_DIM:] + constant


class Plan:
    def __init__(self, sp, tp, rows, context_rows, depth, local):
        self.sp, self.tp, self.chips = sp, tp, tp // 2
        self.block, self.context_rows = rows, context_rows
        self.rows = rows * tp
        self.depth, self.local = depth, local
        heads = local // HEAD_DIM
        self.width = (2 if heads % sp == 0 else 1) * HEAD_DIM
        self.packs = local // self.width
        self.units = 2 * self.packs // sp
        assert self.units in (1, 2) and self.units * sp == 2 * self.packs
        self.half = sp // 2
        self.fold = self.packs // self.half
        assert self.half * 2 == sp and self.fold * self.half == self.packs
        self.group = min(4, self.packs)
        self.groups = self.packs // self.group
        self.pieces = 2 if rows % 32 == 0 else 1
        self.chunk = max(128, local // sp)
        self.owners = local // self.chunk
        self.tile = 512
        self.out_tile = local
        self.out_tiles = depth // self.out_tile
        self.context_blocks = context_rows * sp // BLOCK


def remote(source, target, sent, taken, **peer):
    return pltpu.make_async_remote_copy(
        src_ref=source,
        dst_ref=target,
        send_sem=sent,
        recv_sem=taken,
        device_id=peer,
        device_id_type=MESH,
    )


def layer_kernel(
    plan,
    latent_hbm, context_hbm, condition_ref, context_condition_ref,
    shift_hbm, scale_hbm, gate_hbm, norm_gain_ref,
    decay_down_hbm, decay_up_hbm, rate_down_hbm, rate_up_hbm, bias_ref,
    query_hbm, key_hbm, value_hbm, branch_hbm, group_gain_ref, out_hbm,
    updated_hbm,
    rows_v, context_v, wmod_v, wdown_v, wup_v, wbig_v,
    parts_v, part_in_v, vectors_v, gate_part_v, gate_in_v, gate_all_v, mod_v, inverse_v, normed_v,
    key_v, value_v, decay_v, rate_v, query_v, branch_v, bias_v,
    feature_out_v, feature_in_v, maps_out_v, maps_in_v, reads_q_v, base_v,
    saved_v, cum_v, first_v, transfer_v, constant_v,
    state_out_v, state_in_v, turn_out_v, turn_in_v, entry_out_v, entry_in_v, mixed_v,
    partial_v, pair_v, cross_out_v, cross_in_v, mixer_v,
    local_sem, row_s, row_r, relay_s, relay_r, part_s, part_r, vec_s, vec_r, gp_s, gp_r, gv_s, gv_r,
    feat_s, feat_r, map_s, map_r, st_s, st_r, turn_s, turn_r, ent_s, ent_r, pair_s, pair_r, cross_s, cross_r, store_sem,
):
    sp, tp, chips, width, packs, units = plan.sp, plan.tp, plan.chips, plan.width, plan.packs, plan.units
    depth, local, block = plan.depth, plan.local, plan.block
    half, fold, group, groups = plan.half, plan.fold, plan.group, plan.groups
    me_sp, me_tp = lax.axis_index("sp"), lax.axis_index("tp")
    chip, core = me_tp // 2, lax.rem(me_tp, 2)
    sibling = chip * 2 + 1 - core

    fetches = {}

    def fetch(name, at, source, target):
        copy = pltpu.make_async_copy(source, target, local_sem.at[at])
        copy.start()
        fetches[name] = copy

    fetch("shift", 0, shift_hbm, wmod_v.at[0])
    fetch("scale", 1, scale_hbm, wmod_v.at[1])
    fetch("gate", 2, gate_hbm, wmod_v.at[2])
    fetch("latent", 3, latent_hbm, rows_v.at[me_tp])
    fetch("context", 4, context_hbm, context_v)

    def settle(ref, semaphore):
        remote(ref, ref, semaphore, semaphore, sp=me_sp, tp=me_tp).wait_recv()

    peers = sorted(range(1, sp), key=lambda d: (abs(d - half), d))

    barrier = pltpu.get_barrier_semaphore()
    everyone = [(a, b) for a in range(sp) for b in range(tp) if (a, b) != (0, 0)]
    for a, b in everyone:
        pl.semaphore_signal(
            barrier,
            inc=1,
            device_id={"sp": lax.rem(me_sp + a, sp), "tp": lax.rem(me_tp + b, tp)},
            device_id_type=MESH,
        )

    line = lax.broadcasted_iota(jnp.int32, (8, condition_ref.shape[1]), 0)
    values = jnp.where(line == 0, condition_ref[...], jnp.where(line == 1, context_condition_ref[...], 0.0))
    conditions = (values * jax.nn.sigmoid(values)).astype(BF16)
    shares = []
    for at, name in enumerate(("shift", "scale", "gate")):
        fetches[name].wait()
        shares.append(mm(conditions, wmod_v[at])[0:2])
    fetch("decay_down", 5, decay_down_hbm, wdown_v.at[:, 0 : decay_down_hbm.shape[1]])
    fetch("rate_down", 5, rate_down_hbm, wdown_v.at[:, decay_down_hbm.shape[1] :])
    fetch("key", 7, key_hbm, wbig_v.at[0])
    fetch("value", 8, value_hbm, wbig_v.at[1])
    for j in range(plan.owners):
        c = slice(j * plan.chunk, (j + 1) * plan.chunk)
        parts_v[j, 0:2] = shares[0][:, c]
        parts_v[j, 2:4] = shares[1][:, c]
        gate_part_v[j] = shares[2][0:1, c]

    pl.semaphore_wait(barrier, len(everyone))

    def part_copy(d):
        peer = lax.rem(me_sp + d, sp)
        return peer, remote(
            parts_v.at[peer], part_in_v.at[d - 1], part_s.at[0], part_r.at[0], sp=peer, tp=me_tp
        )

    def gate_copy(d):
        peer = lax.rem(me_sp + d, sp)
        return remote(
            gate_part_v.at[peer], gate_in_v.at[d - 1], gp_s.at[0], gp_r.at[0], sp=peer, tp=me_tp
        )

    def when_owner(at, body):
        if plan.owners == sp:
            body()
        else:
            pl.when(at < plan.owners)(body)

    for d in range(1, sp):
        peer = lax.rem(me_sp + d, sp)
        when_owner(peer, lambda d=d: part_copy(d)[1].start())

    fetches["latent"].wait()

    def slot_of(d, c):
        return lax.rem(chip - d + chips, chips) * 2 + c

    piece = block // plan.pieces

    def row_copy(d, i, slot):
        part = rows_v.at[slot, pl.ds(i * piece, piece)]
        return remote(
            part, part, row_s.at[0], row_r.at[d - 1, i],
            sp=me_sp, tp=lax.rem(chip + d, chips) * 2 + core,
        )

    def relay_copy(d, i, c):
        part = rows_v.at[slot_of(d, c), pl.ds(i * piece, piece)]
        return remote(part, part, relay_s.at[0], relay_r.at[d], sp=me_sp, tp=sibling)

    row_copies = [row_copy(d, i, me_tp) for i in range(plan.pieces) for d in range(1, chips)]
    relay_copies = [relay_copy(d, i, core) for d in range(chips) for i in range(plan.pieces)]
    for copy in row_copies:
        copy.start()
    for i in range(plan.pieces):
        relay_copies[i].start()
    for d in range(1, sp):
        when_owner(lax.rem(me_sp + d, sp), lambda d=d: gate_copy(d).start())

    my_slot = me_tp * plan.owners + me_sp
    vector_copies = [
        remote(
            vectors_v.at[my_slot], vectors_v.at[my_slot], vec_s.at[0], vec_r.at[0],
            sp=lax.rem(me_sp + a, sp), tp=lax.rem(me_tp + b, tp),
        )
        for a, b in everyone
    ]

    def own_columns():
        total = parts_v[me_sp]
        settle(part_in_v, part_r.at[0])
        for d in range(1, sp):
            total = total + part_in_v[d - 1]
        vectors_v[my_slot] = total
        for copy in vector_copies:
            copy.start()

    when_owner(me_sp, own_columns)

    fetch("decay_up", 9, decay_up_hbm, wup_v.at[0])
    fetch("rate_up", 9, rate_up_hbm, wup_v.at[1])
    fetch("query", 11, query_hbm, wbig_v.at[2])
    fetch("branch", 12, branch_hbm, wbig_v.at[3])

    def inverse_of(x):
        x = x.astype(F32)
        mean = jnp.sum(x * x, axis=-1, keepdims=True) * (1.0 / depth)
        return jnp.broadcast_to(lax.rsqrt(mean + NORM_EPS), (16, 128))

    fetches["context"].wait()
    for at in range(0, plan.context_rows, 16):
        inverse_v[(plan.rows + at) // 16] = inverse_of(context_v[at : at + 16])

    def block_inverse(slot):
        for at in range(0, block, 16):
            inverse_v[(slot * block + at) // 16] = inverse_of(rows_v[slot, at : at + 16])

    for p in range(packs):
        bias_v[p] = bias_ref[:, p * width : (p + 1) * width]
    block_inverse(me_tp)
    settle(rows_v.at[sibling], relay_r.at[0])
    block_inverse(sibling)
    for i in range(plan.pieces):
        for d in range(1, chips):
            row_copy(d, i, slot_of(d, core)).wait_recv()
            relay_copies[d * plan.pieces + i].start()
    for d in range(1, chips):
        block_inverse(slot_of(d, core))
    for d in range(1, chips):
        settle(rows_v.at[slot_of(d, 1 - core)], relay_r.at[d])
        block_inverse(slot_of(d, 1 - core))

    def all_but_mine(ref, count, semaphore):
        if plan.owners == sp:
            settle(ref.at[pl.ds(0, count - 1)], semaphore)
        else:
            pl.when(me_sp < plan.owners)(lambda: settle(ref.at[pl.ds(0, count - 1)], semaphore))
            pl.when(me_sp >= plan.owners)(lambda: settle(ref.at[pl.ds(0, count)], semaphore))

    all_but_mine(vectors_v, tp * plan.owners, vec_r.at[0])

    for j in range(tp * plan.owners):
        c = slice(j * plan.chunk, (j + 1) * plan.chunk)
        tile = vectors_v[j]
        mod_v[0:2, c] = norm_gain_ref[:, c] * (1.0 + tile[2:4])
        mod_v[2:4, c] = tile[0:2]

    def modulate(read, group, which):
        inverse = inverse_v[group][:, 0:1]
        for at in range(0, depth, 512):
            c = slice(at, at + 512)
            x = read(c).astype(F32) * inverse * mod_v[which : which + 1, c] + mod_v[2 + which : 3 + which, c]
            normed_v[pl.ds(pl.multiple_of(group * 16, 16), 16), c] = x.astype(BF16)

    per = block // 16

    @pl.loop(0, plan.rows // 16)
    def _(g):
        slot, at = g // per, lax.rem(g, per) * 16
        modulate(lambda c: rows_v[slot, pl.ds(pl.multiple_of(at, 16), 16), c], g, 0)

    for at in range(0, plan.context_rows, 16):
        modulate(lambda c: context_v[at : at + 16, c], (plan.rows + at) // 16, 1)

    rank = decay_down_hbm.shape[1]
    settle(wdown_v, local_sem.at[5])
    settle(wup_v, local_sem.at[9])
    low = sum(
        jnp.dot(normed_v[:, c], wdown_v[c], preferred_element_type=F32)
        for c in (slice(0, depth // 2), slice(depth // 2, depth))
    )
    decay_low = jnp.tanh(low[:, :rank]).astype(BF16)
    rate_low = low[:, rank:].astype(BF16)

    gate_copies = [
        remote(
            gate_all_v.at[my_slot], gate_all_v.at[my_slot], gv_s.at[0], gv_r.at[0],
            sp=lax.rem(me_sp + a, sp), tp=lax.rem(me_tp + b, tp),
        )
        for a, b in everyone
    ]

    def own_gate():
        total = gate_part_v[me_sp]
        settle(gate_in_v, gp_r.at[0])
        for d in range(1, sp):
            total = total + gate_in_v[d - 1]
        gate_all_v[my_slot] = total
        for copy in gate_copies:
            copy.start()

    def spread(found, at, target, kind):
        found = found.astype(BF16)
        for p in range(found.shape[1] // width):
            piece = found[:, p * width : (p + 1) * width]
            target[at // width + p] = piece[: plan.rows]
            if kind is not None:
                feature_out_v[at // width + p, kind] = piece[plan.rows :]

    for name, lhs, which, target, kind in (
        ("decay_up", decay_low, 0, decay_v, 2),
        ("rate_up", rate_low, 1, rate_v, 3),
    ):
        for at in range(0, local, plan.tile):
            found = jnp.dot(lhs, wup_v[which, :, at : at + plan.tile], preferred_element_type=F32)
            spread(found, at, target, kind)

    def project(name, which, rows, target, kind):
        fetches[name].wait()
        for at in range(0, local, plan.tile):
            found = jnp.dot(
                normed_v[0:rows], wbig_v[which, :, at : at + plan.tile], preferred_element_type=F32
            )
            spread(found, at, target, kind)

    def pack_of(d):
        return (d * units) // 2

    def feature_part(at, i):
        return at.at[(pl.ds(2, 2), pl.ds(0, 1), pl.ds(1, 1))[i]]

    def feature_copy(d, i):
        peer = lax.rem(me_sp + d, sp)
        return remote(
            feature_part(feature_out_v.at[pack_of(peer)], i), feature_part(feature_in_v.at[me_sp], i),
            feat_s.at[0], feat_r.at[0], sp=peer, tp=me_tp,
        )

    everything = plan.rows + plan.context_rows
    for d in peers:
        feature_copy(d, 0).start()
    project("key", 0, everything, key_v, 0)
    for d in peers:
        feature_copy(d, 1).start()
    for j in range(plan.out_tiles):
        fetch("out", 6, out_hbm.at[:, j * local : (j + 1) * local], wbig_v.at[0, j * local : (j + 1) * local])
    project("value", 1, everything, value_v, 1)
    for d in peers:
        feature_copy(d, 2).start()
    feature_in_v[me_sp] = feature_out_v[pack_of(me_sp)]
    when_owner(me_sp, own_gate)

    side, index = me_sp // half, lax.rem(me_sp, half)
    blocks = plan.rows // BLOCK

    def map_copy(p):
        owner, slot = p // fold, lax.rem(p, fold)
        d = lax.rem(owner - index + half, half)
        return d, remote(
            maps_out_v.at[p], maps_in_v.at[index, slot], map_s.at[0], map_r.at[0],
            sp=side * half + owner, tp=me_tp,
        )

    def latent_maps(s):
        at = [lax.rem((index + 1) * fold + s * group + i, packs) for i in range(group)]
        items = []
        for p in at:
            k, erase, write, log_decay = chain_inputs(key_v[p], decay_v[p], rate_v[p], bias_v[p])
            items += pack_items(k, value_v[p], erase, write, log_decay, (1, -1))
        found = solve_maps(items, width)
        for i, p in enumerate(at):
            for way in (0, 1):
                mine = found[(i * 2 + way) * blocks : (i * 2 + way + 1) * blocks]
                carried = None
                for b in range(blocks) if way == 0 else reversed(range(blocks)):
                    item = mine[b]
                    transfer, constant = item["transfer"], item["constant"]
                    if carried is not None:
                        first_v[p, way, b, :width] = carried[0].astype(BF16)
                        first_v[p, way, b, width:] = carried[1].astype(BF16)
                        both = mm(jnp.concatenate(carried, axis=0), transfer)
                        transfer, constant = both[:width], both[width:] + constant
                    carried = (transfer, constant)
                    for kind, name in enumerate(("wg", "kg", "response", "offset")):
                        saved_v[p, way, b, kind] = item[name]
                    cum_v[p, way, b] = item["cum"]
                maps_out_v[p, way, 0] = pack_heads(carried[0]).astype(BF16)
                maps_out_v[p, way, 1] = pack_heads(carried[1]).astype(BF16)
            d, copy = map_copy(p)

            @pl.when(d != 0)
            def _(copy=copy):
                copy.start()

    pl.loop(0, groups)(latent_maps)
    for i in range(fold):
        maps_in_v[index, i] = maps_out_v[index * fold + i]

    settle(feature_in_v.at[pl.ds(0, sp - 1)], feat_r.at[0])
    keys, vals, decay_pre, rate_pre = (
        jnp.concatenate([feature_in_v[at, kind] for at in range(sp)], axis=0) for kind in range(4)
    )
    held = pack_of(me_sp)
    k, erase, write, log_decay = chain_inputs(keys, decay_pre, rate_pre, bias_v[held])
    count = plan.context_blocks
    if units == 2:
        ways = (0, 1)
    else:
        ways = (lax.rem(me_sp, 2),)
    found = solve_maps(pack_items(k, vals, erase, write, log_decay, [1 - 2 * way for way in ways]), width)

    def state_copy(u):
        target = ways[u] * half + held // fold
        slot = lax.rem(held, fold)
        return target, slot, remote(
            state_out_v.at[u], state_in_v.at[slot], st_s.at[u], st_r.at[slot], sp=target, tp=me_tp
        )

    for u in range(units):
        mine = found[u * count : (u + 1) * count]
        if units == 2:
            order = mine if u == 0 else mine[::-1]
            state = pack_heads(order[0]["constant"])
            for item in order[1:]:
                state = advance(state, item["transfer"], pack_heads(item["constant"]))
        else:
            for b, item in enumerate(mine):
                transfer_v[b] = item["transfer"].astype(BF16)
                constant_v[b] = pack_heads(item["constant"])
            state = constant_v[jnp.where(ways[0] == 1, count - 1, 0)]
            for step in range(1, count):
                b = jnp.where(ways[0] == 1, count - 1 - step, step)
                state = advance(state, transfer_v[b], constant_v[b])
        state_out_v[u] = state.astype(BF16)
        target, slot, copy = state_copy(u)

        @pl.when(target != me_sp)
        def _(copy=copy):
            copy.start()

        @pl.when(target == me_sp)
        def _(u=u, slot=slot):
            state_in_v[slot] = state_out_v[u]

    project("query", 2, plan.rows, query_v, None)

    def latent_queries(s):
        jobs = []
        for i in range(group):
            p = s * group + i
            for way in (0, 1):
                _, inclusive = signed_masks(1 - 2 * way, width)
                for b in range(blocks):
                    q = query_v[p, b * BLOCK : (b + 1) * BLOCK].astype(F32) * jnp.exp(cum_v[p, way, b])
                    jobs.append({"p": p, "way": way, "b": b, "q": q, "mask": inclusive})
        for job in jobs:
            p, way, b = job["p"], job["way"], job["b"]
            both = mmt(job["q"], above(saved_v[p, way, b, 0], saved_v[p, way, b, 1]))
            job["aw"] = jnp.where(job["mask"], both[:, :width], 0.0)
            job["ak"] = jnp.where(job["mask"], both[:, width:], 0.0)
        for job in jobs:
            p, way, b = job["p"], job["way"], job["b"]
            both = mm(job["aw"], beside(saved_v[p, way, b, 2], saved_v[p, way, b, 3]))
            job["query"] = job["q"] + both[:, :width]
            fed = mm(job["ak"], stack_heads(value_v[p, b * BLOCK : (b + 1) * BLOCK]))
            job["base"] = both[:, width:] + fed
        for job in jobs:
            p, way, b = job["p"], job["way"], job["b"]
            if b != (0 if way == 0 else blocks - 1):
                both = mmt(job["query"], first_v[p, way, b])
                job["query"] = both[:, :width]
                job["base"] = job["base"] + both[:, width:]
            reads_q_v[p, way, b * BLOCK : (b + 1) * BLOCK] = job["query"].astype(BF16)
        for i in range(group):
            mine = jobs[i * 2 * blocks : (i + 1) * 2 * blocks]
            for b in range(blocks):
                base_v[s * group + i, b * BLOCK : (b + 1) * BLOCK] = mine[b]["base"] + mine[blocks + b]["base"]

    def entry_copy(stage, way, at):
        return remote(
            entry_out_v.at[stage, at], entry_in_v.at[way, pl.ds(index * fold, fold)],
            ent_s.at[stage], ent_r.at[stage], sp=side * half + at, tp=me_tp,
        )

    def fold_maps(stage, way, start):
        states = [start[i].astype(F32) for i in range(fold)]
        for step in range(half):
            at = jnp.where(way == 0, step, half - 1 - step)
            for i in range(fold):
                entry_out_v[stage, at, i] = states[i].astype(BF16)

            @pl.when(at != index)
            def _(at=at):
                entry_copy(stage, way, at).start()

            if stage == 0 or step < half - 1:
                for i in range(fold):
                    states[i] = advance(
                        states[i], stack_heads(maps_in_v[at, i, way, 0]), maps_in_v[at, i, way, 1].astype(F32)
                    )
        for i in range(fold):
            entry_in_v[way, index * fold + i] = entry_out_v[stage, index, i]
        return states

    def entries_arrived(stage, way):
        settle(entry_in_v.at[way, pl.ds(0, (half - 1) * fold)], ent_r.at[stage])

    pl.loop(0, groups)(latent_queries)
    settle(maps_in_v.at[pl.ds(0, half - 1)], map_r.at[0])
    for i in range(fold):
        p = index * fold + i

        @pl.when((2 * p + side) // units != me_sp)
        def _(i=i):
            remote(
                state_out_v.at[0], state_in_v.at[i], st_s.at[0], st_r.at[i], sp=me_sp, tp=me_tp
            ).wait_recv()

    states = fold_maps(0, side, state_in_v)
    for i in range(fold):
        turn_out_v[i] = states[i].astype(BF16)
    turn = remote(
        turn_out_v, turn_in_v, turn_s.at[0], turn_r.at[0], sp=(1 - side) * half + index, tp=me_tp
    )
    turn.start()

    project("branch", 3, plan.rows, branch_v, None)
    turn.wait_recv()
    fold_maps(1, 1 - side, turn_in_v)

    entries_arrived(0, side)
    for p in range(packs):
        base_v[p] = base_v[p] + mmt(reads_q_v[p, side], stack_heads(entry_in_v[side, p]))
    entries_arrived(1, 1 - side)

    ones = head_ones(width)
    pair_rows = 2 * block

    def mixed_rows(e):
        at = pl.multiple_of(lax.rem(chip + e, chips) * pair_rows, pair_rows)
        r = pl.ds(at, pair_rows)
        found = [
            base_v[p, r] + mmt(reads_q_v[p, 1 - side, r], stack_heads(entry_in_v[1 - side, p]))
            for p in range(packs)
        ]
        away = [x - group_sum(x, ones, 2) * (1.0 / HEAD_DIM) for x in found]
        variance = [group_sum(x * x, ones, 2) * (1.0 / HEAD_DIM) for x in away]
        for p in range(packs):
            c = slice(p * width, (p + 1) * width)
            gates = branch_v[p, r].astype(F32)
            mixed_v[:, c] = (
                away[p] * lax.rsqrt(variance[p] + GROUP_EPS)
                * group_gain_ref[:, c] * (gates * jax.nn.sigmoid(gates))
            ).astype(BF16)

    def pair_copy(e, j):
        return remote(
            partial_v.at[e, j, 1 - core], pair_v.at[e, j], pair_s.at[0], pair_r.at[(e - 1) * plan.out_tiles + j if e else (chips - 1) * plan.out_tiles],
            sp=me_sp, tp=sibling,
        )

    def cross_copy(e, j):
        return remote(
            cross_out_v.at[e - 1, j], cross_in_v.at[e - 1, j], cross_s.at[0], cross_r.at[e - 1, j],
            sp=me_sp, tp=lax.rem(chip + e, chips) * 2 + core,
        )

    def out_copy(j):
        return pltpu.make_async_copy(
            mixer_v.at[:, j * local : (j + 1) * local], updated_hbm.at[:, j * local : (j + 1) * local], store_sem.at[0]
        )

    settle(wbig_v.at[0], local_sem.at[6])
    for e in [*range(1, chips), 0]:
        mixed_rows(e)
        for j in range(plan.out_tiles):
            found = mm(mixed_v[...], wbig_v[0, j * local : (j + 1) * local]).astype(BF16)
            for i in range(2):
                partial_v[e, j, i] = found[i * block : (i + 1) * block]
            pair_copy(e, j).start()
        if e > 0:
            for j in range(plan.out_tiles):
                pair_copy(e, j).wait_recv()
                cross_out_v[e - 1, j] = (
                    partial_v[e, j, core].astype(F32) + pair_v[e, j].astype(F32)
                ).astype(BF16)
                cross_copy(e, j).start()
    all_but_mine(gate_all_v, tp * plan.owners, gv_r.at[0])
    settle(pair_v.at[0], pair_r.at[(chips - 1) * plan.out_tiles])
    square = jnp.zeros((block, 1), F32)
    totals = []
    for j in range(plan.out_tiles):
        total = partial_v[0, j, core].astype(F32) + pair_v[0, j].astype(F32)
        for e in range(1, chips):
            cross_copy(e, j).wait_recv()
            total = total + cross_in_v[e - 1, j].astype(F32)
        total = total.astype(BF16)
        mixer_v[:, j * local : (j + 1) * local] = total
        total = total.astype(F32)
        square = square + jnp.sum(total * total, axis=-1, keepdims=True)
    inverse = lax.rsqrt(square * (1.0 / depth) + NORM_EPS)
    per_tile = local // plan.chunk
    for j in range(plan.out_tiles):
        for i in range(j * per_tile, (j + 1) * per_tile):
            c = slice(i * plan.chunk, (i + 1) * plan.chunk)
            mixer_v[:, c] = (
                rows_v[me_tp, :, c].astype(F32) + gate_all_v[i] * (mixer_v[:, c].astype(F32) * inverse)
            ).astype(BF16)
        out_copy(j).start()

    all_but_mine(parts_v, plan.owners, part_s.at[0])
    all_but_mine(gate_part_v, plan.owners, gp_s.at[0])
    settle(rows_v.at[pl.ds(0, chips - 1)], row_s.at[0])
    settle(rows_v.at[pl.ds(0, chips)], relay_s.at[0])

    def vectors_left():
        left = len(everyone)
        for ref, semaphore in ((vectors_v, vec_s.at[0]), (gate_all_v, gv_s.at[0])):
            whole, rest = left // ref.shape[0], left % ref.shape[0]
            for _ in range(whole):
                settle(ref, semaphore)
            if rest:
                settle(ref.at[pl.ds(0, rest)], semaphore)

    when_owner(me_sp, vectors_left)
    settle(feature_in_v.at[pl.ds(0, sp - 1)], feat_s.at[0])
    settle(maps_in_v.at[pl.ds(0, half - 1)], map_s.at[0])
    for stage in (0, 1):
        settle(entry_in_v.at[0, pl.ds(0, (half - 1) * fold)], ent_s.at[stage])
    for u in range(units):
        target, _, copy = state_copy(u)

        @pl.when(target != me_sp)
        def _(copy=copy):
            copy.wait_send()

    turn.wait_send()
    settle(pair_v, pair_s.at[0])
    settle(cross_out_v, cross_s.at[0])
    settle(mixer_v, store_sem.at[0])


def on_device(
    latent,
    context,
    condition,
    context_condition,
    shift_weight,
    scale_weight,
    gate_weight,
    norm_gain,
    decay_down,
    decay_up,
    rate_down,
    rate_up,
    head_bias,
    query_weight,
    key_weight,
    value_weight,
    branch_weight,
    group_gain,
    out_weight,
):
    sp, tp = lax.axis_size("sp"), lax.axis_size("tp")
    block, depth = latent.shape
    local = query_weight.shape[1]
    plan = Plan(sp, tp, block, context.shape[0], depth, local)
    width, packs, units, chips = plan.width, plan.packs, plan.units, plan.chips
    rows, crows, tiles = plan.rows, plan.context_rows, plan.out_tiles
    half, fold, blocks = plan.half, plan.fold, rows // BLOCK
    rank = decay_down.shape[1]
    vmem = pl.BlockSpec(memory_space=pltpu.VMEM)
    hbm = pl.BlockSpec(memory_space=pltpu.HBM)
    scratch = [
        ((tp, block, depth), BF16),
        ((crows, depth), BF16),
        ((3, *shift_weight.shape), BF16),
        ((depth, 2 * rank), BF16),
        ((2, rank, local), BF16),
        ((4, depth, local), BF16),
        ((plan.owners, 4, plan.chunk), F32),
        ((sp - 1, 4, plan.chunk), F32),
        ((tp * plan.owners, 4, plan.chunk), F32),
        ((plan.owners, 1, plan.chunk), F32),
        ((sp - 1, 1, plan.chunk), F32),
        ((tp * plan.owners, 1, plan.chunk), F32),
        ((8, depth), F32),
        (((rows + crows) // 16, 16, 128), F32),
        ((rows + crows, depth), BF16),
        ((packs, rows, width), BF16),
        ((packs, rows, width), BF16),
        ((packs, rows, width), BF16),
        ((packs, rows, width), BF16),
        ((packs, rows, width), BF16),
        ((packs, rows, width), BF16),
        ((packs, 2, width), F32),
        ((packs, 4, crows, width), BF16),
        ((sp, 4, crows, width), BF16),
        ((packs, 2, 2, HEAD_DIM, width), BF16),
        ((half, fold, 2, 2, HEAD_DIM, width), BF16),
        ((packs, 2, rows, width), BF16),
        ((packs, rows, width), F32),
        ((packs, 2, blocks, 4, BLOCK, width), BF16),
        ((packs, 2, blocks, BLOCK, width), F32),
        ((packs, 2, blocks, 2 * width, width), BF16),
        ((plan.context_blocks, width, width), BF16),
        ((plan.context_blocks, HEAD_DIM, width), F32),
        ((units, HEAD_DIM, width), BF16),
        ((fold, HEAD_DIM, width), BF16),
        ((fold, HEAD_DIM, width), BF16),
        ((fold, HEAD_DIM, width), BF16),
        ((2, half, fold, HEAD_DIM, width), BF16),
        ((2, packs, HEAD_DIM, width), BF16),
        ((2 * block, local), BF16),
        ((chips, tiles, 2, block, plan.out_tile), BF16),
        ((chips, tiles, block, plan.out_tile), BF16),
        ((chips - 1, tiles, block, plan.out_tile), BF16),
        ((chips - 1, tiles, block, plan.out_tile), BF16),
        ((block, depth), BF16),
    ]
    pieces = plan.pieces
    semaphores = [
        (13,), (1,), (chips - 1, pieces), (1,), (chips,),
        (1,), (1,), (1,), (1,), (1,), (1,), (1,), (1,),
        (1,), (1,), (1,), (1,), (units,), (fold,), (1,), (1,), (2,), (2,),
        (1,), ((chips - 1) * tiles + 1,), (1,), (chips - 1, tiles), (1,),
    ]
    return pl.pallas_call(
        functools.partial(layer_kernel, plan),
        in_specs=[hbm, hbm, vmem, vmem, hbm, hbm, hbm, vmem, hbm, hbm, hbm, hbm, vmem, hbm, hbm, hbm, hbm, vmem, hbm],
        out_specs=hbm,
        out_shape=jax.ShapeDtypeStruct(latent.shape, BF16),
        scratch_shapes=[pltpu.VMEM(shape, kind) for shape, kind in scratch]
        + [pltpu.SemaphoreType.DMA(shape) for shape in semaphores],
        compiler_params=pltpu.CompilerParams(
            collective_id=0, has_side_effects=True, vmem_limit_bytes=VMEM_BYTES
        ),
        name="layer",
    )(
        latent, context, condition.reshape(1, -1), context_condition.reshape(1, -1),
        shift_weight, scale_weight, gate_weight, norm_gain.reshape(1, -1),
        decay_down, decay_up, rate_down, rate_up, head_bias,
        query_weight, key_weight, value_weight, branch_weight, group_gain.reshape(1, -1), out_weight,
    )


def solution(mesh):
    placed = (
        P(("sp", "tp"), None),
        P("sp", None),
        P("sp"),
        P("sp"),
        P("sp", "tp"),
        P("sp", "tp"),
        P("sp", "tp"),
        P(),
        P(),
        P(None, "tp"),
        P(),
        P(None, "tp"),
        P(None, "tp"),
        P(None, "tp"),
        P(None, "tp"),
        P(None, "tp"),
        P(None, "tp"),
        P("tp"),
        P("tp", None),
    )
    return jax.shard_map(
        on_device, mesh=mesh, in_specs=placed, out_specs=P(("sp", "tp"), None), check_vma=False
    )
```

```python
import functools
import math

import jax
import jax.numpy as jnp
from jax import lax
from jax.experimental import pallas as pl
from jax.experimental.pallas import tpu as pltpu
from jax.sharding import PartitionSpec as P

HEAD_DIM = 64
NORM_EPS = 1e-06
GROUP_EPS = 0.00064
DECAY_TOP = math.exp(-0.5)
BLOCK = 64
VMEM_BYTES = 67043328
F32, BF16 = jnp.float32, jnp.bfloat16


def dot_dims(a, b, left, right):
    return lax.dot_general(
        a.astype(BF16), b.astype(BF16), (((left,), (right,)), ((), ())), preferred_element_type=F32
    )


def mm(a, b):
    return dot_dims(a, b, 1, 0)


def mmt(a, b):
    return dot_dims(a, b, 1, 1)


def tmm(a, b):
    return dot_dims(a, b, 0, 0)


def parts_of(x, count):
    found = []
    for _ in range(count):
        part = x.astype(BF16)
        found.append(part)
        x = x - part.astype(F32)
    return found


def head_ones(width):
    row = lax.broadcasted_iota(jnp.int32, (width, width), 0) // HEAD_DIM
    col = lax.broadcasted_iota(jnp.int32, (width, width), 1) // HEAD_DIM
    return (row == col).astype(F32)


def group_sum(x, ones, count=3):
    return sum(mm(part, ones) for part in parts_of(x, count))


def stack_heads(x):
    x = x.astype(BF16)
    count = x.shape[1] // HEAD_DIM
    if count == 1:
        return x
    lane = lax.broadcasted_iota(jnp.int32, (1, x.shape[1]), 1) // HEAD_DIM
    return jnp.concatenate([x * (lane == h).astype(F32).astype(BF16) for h in range(count)], axis=0)


def pack_heads(x):
    return sum(x[at : at + HEAD_DIM] for at in range(0, x.shape[0], HEAD_DIM))


def chain_inputs(keys, decay_pre, rate_pre, head_bias):
    k = keys.astype(F32)
    log_decay = -DECAY_TOP * jax.nn.sigmoid(head_bias[0:1] + decay_pre.astype(F32))
    rate = jax.nn.sigmoid(head_bias[1:2] + rate_pre.astype(F32))
    unit = k * lax.rsqrt(group_sum(k * k, head_ones(k.shape[1]), 2) + 1.0)
    return k, -unit, unit * rate, log_decay


def block_sums(log_decay):
    size = log_decay.shape[0]
    row = lax.broadcasted_iota(jnp.int32, (size, size), 0)
    col = lax.broadcasted_iota(jnp.int32, (size, size), 1)
    mask = ((row >= col) & (row // BLOCK == col // BLOCK)).astype(F32)
    return sum(mm(mask, part) for part in parts_of(log_decay, 3))


def pack_items(k, v, erase, write, log_decay, signs):
    items, ahead = [], block_sums(log_decay)
    for sign in signs:
        for at in range(0, k.shape[0], BLOCK):
            r = slice(at, at + BLOCK)
            total = ahead[at + BLOCK - 1 : at + BLOCK]
            cum = ahead[r]
            if not isinstance(sign, int):
                cum = jnp.where(sign > 0, cum, total - cum + log_decay[r])
            elif sign < 0:
                cum = total - cum + log_decay[r]
            items.append((sign, k[r], v[r], erase[r], write[r], log_decay[r], cum, total))
    return items


def signed_masks(sign, width):
    row = lax.broadcasted_iota(jnp.int32, (BLOCK, width), 0)
    col = lax.broadcasted_iota(jnp.int32, (BLOCK, width), 1) % BLOCK
    return (row - col) * sign > 0, (row - col) * sign >= 0


def beside(left, right):
    return jnp.concatenate([stack_heads(left), stack_heads(right)], axis=1)


def above(left, right):
    return jnp.concatenate([stack_heads(left), stack_heads(right)], axis=0)


def solve_maps(items, width):
    row = lax.broadcasted_iota(jnp.int32, (BLOCK, width), 0)
    col = lax.broadcasted_iota(jnp.int32, (BLOCK, width), 1) % BLOCK
    ones = head_ones(width)
    square = lax.broadcasted_iota(jnp.int32, (width, width), 0)
    unit = (square == lax.broadcasted_iota(jnp.int32, (width, width), 1)).astype(F32)
    one = (row == col).astype(F32)
    near = (row // 2 == col // 2) & (row != col)
    work = []
    for sign, k, v, erase, write, log_decay, cum, total in items:
        strict, _ = signed_masks(sign, width)
        growth = jnp.exp(-cum)
        item = {"es": (erase * jnp.exp(cum - log_decay)).astype(BF16), "v": v.astype(BF16), "cum": cum}
        item["wg"], item["kg"] = (write * growth).astype(BF16), (k * growth).astype(BF16)
        both = mmt(item["es"], above(item["wg"], item["kg"]))
        item["coupling"] = jnp.where(strict, both[:, :width], 0.0)
        item["feed"] = jnp.where(strict, both[:, width:], 0.0)
        tail = jnp.exp(total) * growth
        item["wt"], item["kt"] = (write * tail).astype(BF16), (k * tail).astype(BF16)
        item["diagonal"] = unit * jnp.exp(total)
        work.append(item)
    for item in work:
        item["x"] = one + jnp.where(near, item["coupling"], 0.0)
        item["fed"] = mm(item["feed"], stack_heads(item["v"]))
    size = 2
    while size < BLOCK:
        level = (row // (2 * size) == col // (2 * size)) & (row // size != col // size)
        for item in work:
            item["y"] = mm(jnp.where(level, item["coupling"], 0.0), stack_heads(item["x"]))
        for item in work:
            item["x"] = item["x"] + mm(item["x"], stack_heads(item["y"]))
        size *= 2
    for item in work:
        both = mm(item["x"], beside(item["es"], item["fed"])).astype(BF16)
        item["both"] = both
        item["response"], item["offset"] = both[:, :width], both[:, width:]
    for item in work:
        moved = tmm(item["both"], item["wt"])
        item["transfer"] = moved[:width] * ones + item["diagonal"]
        item["constant"] = (moved[width:] + tmm(item["v"], item["kt"])) * ones
    return work


MESH = pl.DeviceIdType.MESH


def advance(state, transfer, constant):
    high, low = parts_of(state, 2)
    both = mm(jnp.concatenate([high, low], axis=0), transfer)
    return both[:HEAD_DIM] + both[HEAD_DIM:] + constant


class Plan:
    def __init__(self, sp, tp, rows, context_rows, depth, local):
        self.sp, self.tp, self.chips = sp, tp, tp // 2
        self.block, self.context_rows = rows, context_rows
        self.rows = rows * tp
        self.depth, self.local = depth, local
        heads = local // HEAD_DIM
        self.width = (2 if heads % sp == 0 else 1) * HEAD_DIM
        self.packs = local // self.width
        self.units = 2 * self.packs // sp
        assert self.units in (1, 2) and self.units * sp == 2 * self.packs
        self.half = sp // 2
        self.fold = self.packs // self.half
        assert self.half * 2 == sp and self.fold * self.half == self.packs
        self.group = min(4, self.packs)
        self.groups = self.packs // self.group
        self.pieces = 2 if rows % 32 == 0 else 1
        self.chunk = max(128, local // sp)
        self.owners = local // self.chunk
        self.tile = 512
        self.out_tile = local
        self.out_tiles = depth // self.out_tile
        self.context_blocks = context_rows * sp // BLOCK


def remote(source, target, sent, taken, **peer):
    return pltpu.make_async_remote_copy(
        src_ref=source,
        dst_ref=target,
        send_sem=sent,
        recv_sem=taken,
        device_id=peer,
        device_id_type=MESH,
    )


def layer_kernel(
    plan,
    latent_hbm, context_hbm, condition_hbm, context_condition_hbm,
    shift_hbm, scale_hbm, gate_hbm, norm_gain_hbm,
    decay_down_hbm, decay_up_hbm, rate_down_hbm, rate_up_hbm, bias_hbm,
    query_hbm, key_hbm, value_hbm, branch_hbm, group_gain_hbm, out_hbm,
    updated_hbm,
    condition_v, norm_gain_ref, bias_ref, group_gain_ref, rows_v, context_v, wmod_v, wdown_v, wup_v, wbig_v,
    parts_v, part_in_v, vectors_v, gate_part_v, gate_in_v, gate_all_v, mod_v, inverse_v, normed_v,
    key_v, value_v, decay_v, rate_v, query_v, branch_v, bias_v,
    feature_out_v, feature_in_v, maps_out_v, maps_in_v, reads_q_v, base_v,
    saved_v, cum_v, first_v, transfer_v, constant_v,
    prefix_v, state_out_v, state_in_v, turn_out_v, turn_in_v, entry_out_v, entry_in_v, mixed_v,
    partial_v, pair_v, cross_out_v, cross_in_v, mixer_v,
    local_sem, row_s, row_r, relay_s, relay_r, part_s, part_r, vec_s, vec_r, gp_s, gp_r, gv_s, gv_r,
    feat_s, feat_r, map_s, map_r, st_s, st_r, turn_s, turn_r, ent_s, ent_r, pair_s, pair_r, cross_s, cross_r, store_sem,
):
    sp, tp, chips, width, packs, units = plan.sp, plan.tp, plan.chips, plan.width, plan.packs, plan.units
    depth, local, block = plan.depth, plan.local, plan.block
    half, fold, group, groups = plan.half, plan.fold, plan.group, plan.groups
    me_sp, me_tp = lax.axis_index("sp"), lax.axis_index("tp")
    chip, core = me_tp // 2, lax.rem(me_tp, 2)
    sibling = chip * 2 + 1 - core

    fetches = {}

    def fetch(name, at, source, target):
        copy = pltpu.make_async_copy(source, target, local_sem.at[at])
        copy.start()
        fetches[name] = copy

    def settle(ref, semaphore):
        remote(ref, ref, semaphore, semaphore, sp=me_sp, tp=me_tp).wait_recv()

    peers = sorted(range(1, sp), key=lambda d: (abs(d - half), d))

    barrier = pltpu.get_barrier_semaphore()
    everyone = [(a, b) for a in (*peers, 0) for b in reversed(range(tp)) if (a, b) != (0, 0)]
    greeted = [(a, b) for a, b in everyone if a == 0 or b == 0]
    for a, b in greeted:
        pl.semaphore_signal(
            barrier,
            inc=1,
            device_id={"sp": lax.rem(me_sp + a, sp), "tp": lax.rem(me_tp + b, tp)},
            device_id_type=MESH,
        )

    fetch("condition", 10, condition_hbm, condition_v.at[0])
    fetch("context_condition", 10, context_condition_hbm, condition_v.at[1])
    fetch("shift", 0, shift_hbm, wmod_v.at[0])
    fetch("scale", 1, scale_hbm, wmod_v.at[1])
    fetch("latent", 3, latent_hbm, rows_v.at[me_tp])
    fetch("context", 4, context_hbm, context_v)
    fetch("norm_gain", 13, norm_gain_hbm, norm_gain_ref)
    fetch("bias", 14, bias_hbm, bias_ref)
    fetch("group_gain", 15, group_gain_hbm, group_gain_ref)

    line = lax.broadcasted_iota(jnp.int32, (8, condition_v.shape[2]), 0)
    settle(condition_v, local_sem.at[10])
    values = jnp.where(line == 0, condition_v[0], jnp.where(line == 1, condition_v[1], 0.0))
    conditions = (values * jax.nn.sigmoid(values)).astype(BF16)
    for at, name in enumerate(("shift", "scale")):
        fetches[name].wait()
        share = mm(conditions, wmod_v[at])[0:2]
        for j in range(plan.owners):
            parts_v[j, 2 * at : 2 * at + 2] = share[:, j * plan.chunk : (j + 1) * plan.chunk]

    pl.semaphore_wait(barrier, len(greeted))

    def part_copy(d):
        peer = lax.rem(me_sp + d, sp)
        return peer, remote(
            parts_v.at[peer], part_in_v.at[d - 1], part_s.at[0], part_r.at[0], sp=peer, tp=me_tp
        )

    def gate_copy(d):
        peer = lax.rem(me_sp + d, sp)
        return remote(
            gate_part_v.at[peer], gate_in_v.at[d - 1], gp_s.at[0], gp_r.at[0], sp=peer, tp=me_tp
        )

    def when_owner(at, body):
        if plan.owners == sp:
            body()
        else:
            pl.when(at < plan.owners)(body)

    for d in peers:
        peer = lax.rem(me_sp + d, sp)
        when_owner(peer, lambda d=d: part_copy(d)[1].start())

    fetches["latent"].wait()

    def slot_of(d, c):
        return lax.rem(chip - d + chips, chips) * 2 + c

    piece = block // plan.pieces

    def row_copy(d, i, slot):
        part = rows_v.at[slot, pl.ds(i * piece, piece)]
        return remote(
            part, part, row_s.at[0], row_r.at[d - 1, i],
            sp=me_sp, tp=lax.rem(chip + d, chips) * 2 + core,
        )

    def relay_copy(d, i, c):
        part = rows_v.at[slot_of(d, c), pl.ds(i * piece, piece)]
        return remote(part, part, relay_s.at[0], relay_r.at[d], sp=me_sp, tp=sibling)

    row_copies = [row_copy(d, i, me_tp) for i in range(plan.pieces) for d in range(1, chips)]
    relay_copies = [relay_copy(d, i, core) for d in range(chips) for i in range(plan.pieces)]
    for copy in row_copies:
        copy.start()
    for i in range(plan.pieces):
        relay_copies[i].start()
    fetch("gate", 2, gate_hbm, wmod_v.at[2])
    fetch("decay_down", 5, decay_down_hbm, wdown_v.at[:, 0 : decay_down_hbm.shape[1]])
    fetch("rate_down", 5, rate_down_hbm, wdown_v.at[:, decay_down_hbm.shape[1] :])
    fetch("key", 7, key_hbm, wbig_v.at[0])
    fetch("value", 8, value_hbm, wbig_v.at[1])

    my_slot = me_tp * plan.owners + me_sp
    vector_copies = [
        remote(
            vectors_v.at[my_slot], vectors_v.at[my_slot], vec_s.at[0], vec_r.at[0],
            sp=lax.rem(me_sp + a, sp), tp=lax.rem(me_tp + b, tp),
        )
        for a, b in everyone
    ]

    def own_columns():
        total = parts_v[me_sp]
        settle(part_in_v, part_r.at[0])
        for d in range(1, sp):
            total = total + part_in_v[d - 1]
        vectors_v[my_slot] = total
        for copy in vector_copies:
            copy.start()

    when_owner(me_sp, own_columns)

    fetch("decay_up", 9, decay_up_hbm, wup_v.at[0])
    fetch("rate_up", 9, rate_up_hbm, wup_v.at[1])
    fetch("query", 11, query_hbm, wbig_v.at[2])
    fetch("branch", 12, branch_hbm, wbig_v.at[3])

    fetches["gate"].wait()
    share = mm(conditions, wmod_v[2])[0:1]
    for j in range(plan.owners):
        gate_part_v[j] = share[:, j * plan.chunk : (j + 1) * plan.chunk]
    for d in peers:
        when_owner(lax.rem(me_sp + d, sp), lambda d=d: gate_copy(d).start())

    def inverse_of(x):
        x = x.astype(F32)
        mean = jnp.sum(x * x, axis=-1, keepdims=True) * (1.0 / depth)
        return jnp.broadcast_to(lax.rsqrt(mean + NORM_EPS), (16, 128))

    fetches["context"].wait()
    for at in range(0, plan.context_rows, 16):
        inverse_v[(plan.rows + at) // 16] = inverse_of(context_v[at : at + 16])

    def block_inverse(slot):
        for at in range(0, block, 16):
            inverse_v[(slot * block + at) // 16] = inverse_of(rows_v[slot, at : at + 16])

    for name in ("norm_gain", "bias", "group_gain"):
        fetches[name].wait()
    for p in range(packs):
        bias_v[p] = bias_ref[:, p * width : (p + 1) * width]
    block_inverse(me_tp)
    settle(rows_v.at[sibling], relay_r.at[0])
    block_inverse(sibling)
    for i in range(plan.pieces):
        for d in range(1, chips):
            row_copy(d, i, slot_of(d, core)).wait_recv()
            relay_copies[d * plan.pieces + i].start()
    for d in range(1, chips):
        block_inverse(slot_of(d, core))
    for d in range(1, chips):
        settle(rows_v.at[slot_of(d, 1 - core)], relay_r.at[d])
        block_inverse(slot_of(d, 1 - core))

    def all_but_mine(ref, count, semaphore):
        if plan.owners == sp:
            settle(ref.at[pl.ds(0, count - 1)], semaphore)
        else:
            pl.when(me_sp < plan.owners)(lambda: settle(ref.at[pl.ds(0, count - 1)], semaphore))
            pl.when(me_sp >= plan.owners)(lambda: settle(ref.at[pl.ds(0, count)], semaphore))

    all_but_mine(vectors_v, tp * plan.owners, vec_r.at[0])

    for j in range(tp * plan.owners):
        c = slice(j * plan.chunk, (j + 1) * plan.chunk)
        tile = vectors_v[j]
        mod_v[0:2, c] = norm_gain_ref[:, c] * (1.0 + tile[2:4])
        mod_v[2:4, c] = tile[0:2]

    def modulate(read, group, which):
        inverse = inverse_v[group][:, 0:1]
        for at in range(0, depth, 512):
            c = slice(at, at + 512)
            x = read(c).astype(F32) * inverse * mod_v[which : which + 1, c] + mod_v[2 + which : 3 + which, c]
            normed_v[pl.ds(pl.multiple_of(group * 16, 16), 16), c] = x.astype(BF16)

    per = block // 16

    @pl.loop(0, plan.rows // 16, unroll=2)
    def _(g):
        slot, at = g // per, lax.rem(g, per) * 16
        modulate(lambda c: rows_v[slot, pl.ds(pl.multiple_of(at, 16), 16), c], g, 0)

    for at in range(0, plan.context_rows, 16):
        modulate(lambda c: context_v[at : at + 16, c], (plan.rows + at) // 16, 1)

    rank = decay_down_hbm.shape[1]
    settle(wdown_v, local_sem.at[5])
    settle(wup_v, local_sem.at[9])
    fetches["key"].wait()
    fetches["value"].wait()
    low = sum(
        jnp.dot(normed_v[:, c], wdown_v[c], preferred_element_type=F32)
        for c in (slice(0, depth // 2), slice(depth // 2, depth))
    )
    gate_copies = [
        remote(
            gate_all_v.at[my_slot], gate_all_v.at[my_slot], gv_s.at[0], gv_r.at[0],
            sp=lax.rem(me_sp + a, sp), tp=lax.rem(me_tp + b, tp),
        )
        for a, b in everyone
    ]

    def own_gate():
        total = gate_part_v[me_sp]
        settle(gate_in_v, gp_r.at[0])
        for d in range(1, sp):
            total = total + gate_in_v[d - 1]
        gate_all_v[my_slot] = total
        for copy in gate_copies:
            copy.start()

    def spread(found, at, target, kind):
        found = found.astype(BF16)
        for p in range(found.shape[1] // width):
            piece = found[:, p * width : (p + 1) * width]
            target[at // width + p] = piece[: plan.rows]
            if kind is not None:
                feature_out_v[at // width + p, kind] = piece[plan.rows :]

    def project(which, rows, target, kind, tiles):
        for at in tiles:
            found = jnp.dot(
                normed_v[0:rows], wbig_v[which, :, at : at + plan.tile], preferred_element_type=F32
            )
            spread(found, at, target, kind)

    def pack_of(d):
        return (d * units) // 2

    def feature_part(at, i):
        return at.at[(pl.ds(2, 2), pl.ds(0, 1), pl.ds(1, 1))[i]]

    def feature_copy(d, i):
        peer = lax.rem(me_sp + d, sp)
        return remote(
            feature_part(feature_out_v.at[pack_of(peer)], i), feature_part(feature_in_v.at[me_sp], i),
            feat_s.at[0], feat_r.at[0], sp=peer, tp=me_tp,
        )

    everything = plan.rows + plan.context_rows
    tiles = list(range(0, local, plan.tile))
    project(0, everything, key_v, 0, tiles[:1])
    decay_low = jnp.tanh(low[:, :rank]).astype(BF16)
    rate_low = low[:, rank:].astype(BF16)

    for name, lhs, which, target, kind in (
        ("decay_up", decay_low, 0, decay_v, 2),
        ("rate_up", rate_low, 1, rate_v, 3),
    ):
        for at in range(0, local, plan.tile):
            found = jnp.dot(lhs, wup_v[which, :, at : at + plan.tile], preferred_element_type=F32)
            spread(found, at, target, kind)
    for d in peers:
        feature_copy(d, 0).start()
    project(0, everything, key_v, 0, tiles[1:])
    for d in peers:
        feature_copy(d, 1).start()
    for j in range(plan.out_tiles):
        fetch("out", 6, out_hbm.at[:, j * local : (j + 1) * local], wbig_v.at[0, j * local : (j + 1) * local])
    project(1, everything, value_v, 1, tiles)
    for d in peers:
        feature_copy(d, 2).start()
    feature_in_v[me_sp] = feature_out_v[pack_of(me_sp)]
    when_owner(me_sp, own_gate)

    side, index = me_sp // half, lax.rem(me_sp, half)
    blocks = plan.rows // BLOCK

    def map_copy(p):
        owner, slot = p // fold, lax.rem(p, fold)
        d = lax.rem(owner - index + half, half)
        return d, remote(
            maps_out_v.at[p], maps_in_v.at[index, slot], map_s.at[0], map_r.at[0],
            sp=side * half + owner, tp=me_tp,
        )

    def latent_maps(s):
        at = [lax.rem((index + 1) * fold + s * group + i, packs) for i in range(group)]
        items = []
        for p in at:
            k, erase, write, log_decay = chain_inputs(key_v[p], decay_v[p], rate_v[p], bias_v[p])
            items += pack_items(k, value_v[p], erase, write, log_decay, (1, -1))
        found = solve_maps(items, width)
        for i, p in enumerate(at):
            for way in (0, 1):
                mine = found[(i * 2 + way) * blocks : (i * 2 + way + 1) * blocks]
                carried = None
                for b in range(blocks) if way == 0 else reversed(range(blocks)):
                    item = mine[b]
                    transfer, constant = item["transfer"], item["constant"]
                    if carried is not None:
                        first_v[p, way, b, :width] = carried[0].astype(BF16)
                        first_v[p, way, b, width:] = carried[1].astype(BF16)
                        both = mm(jnp.concatenate(carried, axis=0), transfer)
                        transfer, constant = both[:width], both[width:] + constant
                    carried = (transfer, constant)
                    for kind, name in enumerate(("wg", "kg", "response", "offset")):
                        saved_v[p, way, b, kind] = item[name]
                    cum_v[p, way, b] = item["cum"]
                maps_out_v[p, way, 0] = pack_heads(carried[0]).astype(BF16)
                maps_out_v[p, way, 1] = pack_heads(carried[1]).astype(BF16)
            d, copy = map_copy(p)

            @pl.when(d != 0)
            def _(copy=copy):
                copy.start()

    pl.loop(0, groups)(latent_maps)
    for i in range(fold):
        maps_in_v[index, i] = maps_out_v[index * fold + i]

    settle(feature_in_v.at[pl.ds(0, sp - 1)], feat_r.at[0])
    keys, vals, decay_pre, rate_pre = (
        jnp.concatenate([feature_in_v[at, kind] for at in range(sp)], axis=0) for kind in range(4)
    )
    held = pack_of(me_sp)
    k, erase, write, log_decay = chain_inputs(keys, decay_pre, rate_pre, bias_v[held])
    count = plan.context_blocks
    if units == 2:
        ways = (0, 1)
    else:
        ways = (lax.rem(me_sp, 2),)
    found = solve_maps(pack_items(k, vals, erase, write, log_decay, [1 - 2 * way for way in ways]), width)

    def state_copy(u):
        target = ways[u] * half + held // fold
        slot = lax.rem(held, fold)
        return target, slot, remote(
            state_out_v.at[u], state_in_v.at[slot], st_s.at[u], st_r.at[slot], sp=target, tp=me_tp
        )

    for u in range(units):
        mine = found[u * count : (u + 1) * count]
        if units == 2:
            order = mine if u == 0 else mine[::-1]
            state = pack_heads(order[0]["constant"])
            for item in order[1:]:
                state = advance(state, item["transfer"], pack_heads(item["constant"]))
        else:
            for b, item in enumerate(mine):
                transfer_v[b] = item["transfer"].astype(BF16)
                constant_v[b] = pack_heads(item["constant"])
            state = constant_v[jnp.where(ways[0] == 1, count - 1, 0)]
            for step in range(1, count):
                b = jnp.where(ways[0] == 1, count - 1 - step, step)
                state = advance(state, transfer_v[b], constant_v[b])
        state_out_v[u] = state.astype(BF16)
        target, slot, copy = state_copy(u)

        @pl.when(target != me_sp)
        def _(copy=copy):
            copy.start()

        @pl.when(target == me_sp)
        def _(u=u, slot=slot):
            state_in_v[slot] = state_out_v[u]

    fetches["query"].wait()
    project(2, plan.rows, query_v, None, tiles)

    def latent_queries(s):
        jobs = []
        for i in range(group):
            p = s * group + i
            for way in (0, 1):
                _, inclusive = signed_masks(1 - 2 * way, width)
                for b in range(blocks):
                    q = query_v[p, b * BLOCK : (b + 1) * BLOCK].astype(F32) * jnp.exp(cum_v[p, way, b])
                    jobs.append({"p": p, "way": way, "b": b, "q": q, "mask": inclusive})
        for job in jobs:
            p, way, b = job["p"], job["way"], job["b"]
            both = mmt(job["q"], above(saved_v[p, way, b, 0], saved_v[p, way, b, 1]))
            job["aw"] = jnp.where(job["mask"], both[:, :width], 0.0)
            job["ak"] = jnp.where(job["mask"], both[:, width:], 0.0)
        for job in jobs:
            p, way, b = job["p"], job["way"], job["b"]
            both = mm(job["aw"], beside(saved_v[p, way, b, 2], saved_v[p, way, b, 3]))
            job["query"] = job["q"] + both[:, :width]
            fed = mm(job["ak"], stack_heads(value_v[p, b * BLOCK : (b + 1) * BLOCK]))
            job["base"] = both[:, width:] + fed
        for job in jobs:
            p, way, b = job["p"], job["way"], job["b"]
            if b != (0 if way == 0 else blocks - 1):
                both = mmt(job["query"], first_v[p, way, b])
                job["query"] = both[:, :width]
                job["base"] = job["base"] + both[:, width:]
            reads_q_v[p, way, b * BLOCK : (b + 1) * BLOCK] = job["query"].astype(BF16)
        for i in range(group):
            mine = jobs[i * 2 * blocks : (i + 1) * 2 * blocks]
            for b in range(blocks):
                base_v[s * group + i, b * BLOCK : (b + 1) * BLOCK] = mine[b]["base"] + mine[blocks + b]["base"]

    def entry_copy(stage, way, at):
        return remote(
            entry_out_v.at[stage, at], entry_in_v.at[way, pl.ds(index * fold, fold)],
            ent_s.at[stage], ent_r.at[stage], sp=side * half + at, tp=me_tp,
        )

    def place(way, step):
        return jnp.where(way == 0, step, half - 1 - step)

    def compose_maps(way):
        for i in range(fold):
            found = maps_in_v[place(way, 0), i, way]
            both = jnp.concatenate([found[0].astype(F32), found[1].astype(F32)], axis=0)
            prefix_v[way, i, 0] = both.astype(BF16)
            for step in range(1, half):
                found = maps_in_v[place(way, step), i, way]
                both = mm(both, stack_heads(found[0]))
                both = jnp.concatenate([both[:HEAD_DIM], both[HEAD_DIM:] + found[1].astype(F32)], axis=0)
                prefix_v[way, i, step] = both.astype(BF16)

    def moved(way, i, step, state):
        found = prefix_v[way, i, step]
        return advance(state, stack_heads(found[:HEAD_DIM]), found[HEAD_DIM:].astype(F32))

    def fold_maps(stage, way, start):
        states = [start[i].astype(F32) for i in range(fold)]
        for i in range(fold):
            entry_out_v[stage, place(way, 0), i] = start[i]
        for step in range(1, half):
            for i in range(fold):
                entry_out_v[stage, place(way, step), i] = moved(way, i, step - 1, states[i]).astype(BF16)
        for d in range(1, half):
            entry_copy(stage, way, lax.rem(index + d, half)).start()
        for i in range(fold):
            entry_in_v[way, index * fold + i] = entry_out_v[stage, index, i]

    def entries_arrived(stage, way):
        settle(entry_in_v.at[way, pl.ds(0, (half - 1) * fold)], ent_r.at[stage])

    settle(maps_in_v.at[pl.ds(0, half - 1)], map_r.at[0])
    for way in (0, 1):
        compose_maps(way)
    for i in range(fold):
        p = index * fold + i

        @pl.when((2 * p + side) // units != me_sp)
        def _(i=i):
            remote(
                state_out_v.at[0], state_in_v.at[i], st_s.at[0], st_r.at[i], sp=me_sp, tp=me_tp
            ).wait_recv()

    for i in range(fold):
        turn_out_v[i] = moved(side, i, half - 1, state_in_v[i].astype(F32)).astype(BF16)
    turn = remote(
        turn_out_v, turn_in_v, turn_s.at[0], turn_r.at[0], sp=(1 - side) * half + index, tp=me_tp
    )
    turn.start()
    fold_maps(0, side, state_in_v)
    pl.loop(0, groups)(latent_queries)

    fetches["branch"].wait()
    project(3, plan.rows, branch_v, None, tiles)
    turn.wait_recv()
    fold_maps(1, 1 - side, turn_in_v)

    entries_arrived(0, side)
    for p in range(packs):
        base_v[p] = base_v[p] + mmt(reads_q_v[p, side], stack_heads(entry_in_v[side, p]))
    entries_arrived(1, 1 - side)

    ones = head_ones(width)
    pair_rows = 2 * block

    def mixed_rows(e):
        at = pl.multiple_of(lax.rem(chip + e, chips) * pair_rows, pair_rows)
        r = pl.ds(at, pair_rows)
        found = [
            base_v[p, r] + mmt(reads_q_v[p, 1 - side, r], stack_heads(entry_in_v[1 - side, p]))
            for p in range(packs)
        ]
        away = [x - group_sum(x, ones, 2) * (1.0 / HEAD_DIM) for x in found]
        variance = [group_sum(x * x, ones, 2) * (1.0 / HEAD_DIM) for x in away]
        for p in range(packs):
            c = slice(p * width, (p + 1) * width)
            gates = branch_v[p, r].astype(F32)
            mixed_v[:, c] = (
                away[p] * lax.rsqrt(variance[p] + GROUP_EPS)
                * group_gain_ref[:, c] * (gates * jax.nn.sigmoid(gates))
            ).astype(BF16)

    def pair_copy(e, j):
        return remote(
            partial_v.at[e, j, 1 - core], pair_v.at[e, j], pair_s.at[0], pair_r.at[(e - 1) * plan.out_tiles + j if e else (chips - 1) * plan.out_tiles],
            sp=me_sp, tp=sibling,
        )

    def cross_copy(e, j):
        return remote(
            cross_out_v.at[e - 1, j], cross_in_v.at[e - 1, j], cross_s.at[0], cross_r.at[e - 1, j],
            sp=me_sp, tp=lax.rem(chip + e, chips) * 2 + core,
        )

    def out_copy(j):
        return pltpu.make_async_copy(
            mixer_v.at[:, j * local : (j + 1) * local], updated_hbm.at[:, j * local : (j + 1) * local], store_sem.at[0]
        )

    settle(wbig_v.at[0], local_sem.at[6])
    for e in [*range(1, chips), 0]:
        mixed_rows(e)
        for j in range(plan.out_tiles):
            found = mm(mixed_v[...], wbig_v[0, j * local : (j + 1) * local]).astype(BF16)
            for i in range(2):
                partial_v[e, j, i] = found[i * block : (i + 1) * block]
            pair_copy(e, j).start()
        if e > 0:
            for j in range(plan.out_tiles):
                pair_copy(e, j).wait_recv()
                cross_out_v[e - 1, j] = (
                    partial_v[e, j, core].astype(F32) + pair_v[e, j].astype(F32)
                ).astype(BF16)
                cross_copy(e, j).start()
    all_but_mine(gate_all_v, tp * plan.owners, gv_r.at[0])
    settle(pair_v.at[0], pair_r.at[(chips - 1) * plan.out_tiles])
    square = jnp.zeros((block, 1), F32)
    totals = []
    for j in range(plan.out_tiles):
        total = partial_v[0, j, core].astype(F32) + pair_v[0, j].astype(F32)
        for e in range(1, chips):
            cross_copy(e, j).wait_recv()
            total = total + cross_in_v[e - 1, j].astype(F32)
        total = total.astype(BF16)
        mixer_v[:, j * local : (j + 1) * local] = total
        total = total.astype(F32)
        square = square + jnp.sum(total * total, axis=-1, keepdims=True)
    inverse = lax.rsqrt(square * (1.0 / depth) + NORM_EPS)
    per_tile = local // plan.chunk
    for j in range(plan.out_tiles):
        for i in range(j * per_tile, (j + 1) * per_tile):
            c = slice(i * plan.chunk, (i + 1) * plan.chunk)
            mixer_v[:, c] = (
                rows_v[me_tp, :, c].astype(F32) + gate_all_v[i] * (mixer_v[:, c].astype(F32) * inverse)
            ).astype(BF16)
        out_copy(j).start()

    all_but_mine(parts_v, plan.owners, part_s.at[0])
    all_but_mine(gate_part_v, plan.owners, gp_s.at[0])
    settle(rows_v.at[pl.ds(0, chips - 1)], row_s.at[0])
    settle(rows_v.at[pl.ds(0, chips)], relay_s.at[0])

    def vectors_left():
        left = len(everyone)
        for ref, semaphore in ((vectors_v, vec_s.at[0]), (gate_all_v, gv_s.at[0])):
            whole, rest = left // ref.shape[0], left % ref.shape[0]
            for _ in range(whole):
                settle(ref, semaphore)
            if rest:
                settle(ref.at[pl.ds(0, rest)], semaphore)

    when_owner(me_sp, vectors_left)
    settle(feature_in_v.at[pl.ds(0, sp - 1)], feat_s.at[0])
    settle(maps_in_v.at[pl.ds(0, half - 1)], map_s.at[0])
    for stage in (0, 1):
        settle(entry_in_v.at[0, pl.ds(0, (half - 1) * fold)], ent_s.at[stage])
    for u in range(units):
        target, _, copy = state_copy(u)

        @pl.when(target != me_sp)
        def _(copy=copy):
            copy.wait_send()

    turn.wait_send()
    settle(pair_v, pair_s.at[0])
    settle(cross_out_v, cross_s.at[0])
    settle(mixer_v, store_sem.at[0])


def on_device(
    latent,
    context,
    condition,
    context_condition,
    shift_weight,
    scale_weight,
    gate_weight,
    norm_gain,
    decay_down,
    decay_up,
    rate_down,
    rate_up,
    head_bias,
    query_weight,
    key_weight,
    value_weight,
    branch_weight,
    group_gain,
    out_weight,
):
    sp, tp = lax.axis_size("sp"), lax.axis_size("tp")
    block, depth = latent.shape
    local = query_weight.shape[1]
    plan = Plan(sp, tp, block, context.shape[0], depth, local)
    width, packs, units, chips = plan.width, plan.packs, plan.units, plan.chips
    rows, crows, tiles = plan.rows, plan.context_rows, plan.out_tiles
    half, fold, blocks = plan.half, plan.fold, rows // BLOCK
    rank = decay_down.shape[1]
    hbm = pl.BlockSpec(memory_space=pltpu.HBM)
    scratch = [
        ((2, 1, condition.shape[0]), F32),
        ((1, depth), F32),
        ((2, local), F32),
        ((1, local), F32),
        ((tp, block, depth), BF16),
        ((crows, depth), BF16),
        ((3, *shift_weight.shape), BF16),
        ((depth, 2 * rank), BF16),
        ((2, rank, local), BF16),
        ((4, depth, local), BF16),
        ((plan.owners, 4, plan.chunk), F32),
        ((sp - 1, 4, plan.chunk), F32),
        ((tp * plan.owners, 4, plan.chunk), F32),
        ((plan.owners, 1, plan.chunk), F32),
        ((sp - 1, 1, plan.chunk), F32),
        ((tp * plan.owners, 1, plan.chunk), F32),
        ((8, depth), F32),
        (((rows + crows) // 16, 16, 128), F32),
        ((rows + crows, depth), BF16),
        ((packs, rows, width), BF16),
        ((packs, rows, width), BF16),
        ((packs, rows, width), BF16),
        ((packs, rows, width), BF16),
        ((packs, rows, width), BF16),
        ((packs, rows, width), BF16),
        ((packs, 2, width), F32),
        ((packs, 4, crows, width), BF16),
        ((sp, 4, crows, width), BF16),
        ((packs, 2, 2, HEAD_DIM, width), BF16),
        ((half, fold, 2, 2, HEAD_DIM, width), BF16),
        ((packs, 2, rows, width), BF16),
        ((packs, rows, width), F32),
        ((packs, 2, blocks, 4, BLOCK, width), BF16),
        ((packs, 2, blocks, BLOCK, width), F32),
        ((packs, 2, blocks, 2 * width, width), BF16),
        ((plan.context_blocks, width, width), BF16),
        ((plan.context_blocks, HEAD_DIM, width), F32),
        ((2, fold, half, 2 * HEAD_DIM, width), BF16),
        ((units, HEAD_DIM, width), BF16),
        ((fold, HEAD_DIM, width), BF16),
        ((fold, HEAD_DIM, width), BF16),
        ((fold, HEAD_DIM, width), BF16),
        ((2, half, fold, HEAD_DIM, width), BF16),
        ((2, packs, HEAD_DIM, width), BF16),
        ((2 * block, local), BF16),
        ((chips, tiles, 2, block, plan.out_tile), BF16),
        ((chips, tiles, block, plan.out_tile), BF16),
        ((chips - 1, tiles, block, plan.out_tile), BF16),
        ((chips - 1, tiles, block, plan.out_tile), BF16),
        ((block, depth), BF16),
    ]
    pieces = plan.pieces
    semaphores = [
        (16,), (1,), (chips - 1, pieces), (1,), (chips,),
        (1,), (1,), (1,), (1,), (1,), (1,), (1,), (1,),
        (1,), (1,), (1,), (1,), (units,), (fold,), (1,), (1,), (2,), (2,),
        (1,), ((chips - 1) * tiles + 1,), (1,), (chips - 1, tiles), (1,),
    ]
    return pl.pallas_call(
        functools.partial(layer_kernel, plan),
        in_specs=[hbm] * 19,
        out_specs=hbm,
        out_shape=jax.ShapeDtypeStruct(latent.shape, BF16),
        scratch_shapes=[pltpu.VMEM(shape, kind) for shape, kind in scratch]
        + [pltpu.SemaphoreType.DMA(shape) for shape in semaphores],
        compiler_params=pltpu.CompilerParams(
            collective_id=0, has_side_effects=True, vmem_limit_bytes=VMEM_BYTES
        ),
        name="layer",
    )(
        latent, context, condition.reshape(1, -1), context_condition.reshape(1, -1),
        shift_weight, scale_weight, gate_weight, norm_gain.reshape(1, -1),
        decay_down, decay_up, rate_down, rate_up, head_bias,
        query_weight, key_weight, value_weight, branch_weight, group_gain.reshape(1, -1), out_weight,
    )


def solution(mesh):
    placed = (
        P(("sp", "tp"), None),
        P("sp", None),
        P("sp"),
        P("sp"),
        P("sp", "tp"),
        P("sp", "tp"),
        P("sp", "tp"),
        P(),
        P(),
        P(None, "tp"),
        P(),
        P(None, "tp"),
        P(None, "tp"),
        P(None, "tp"),
        P(None, "tp"),
        P(None, "tp"),
        P(None, "tp"),
        P("tp"),
        P("tp", None),
    )
    return jax.shard_map(
        on_device, mesh=mesh, in_specs=placed, out_specs=P(("sp", "tp"), None), check_vma=False
    )
```

```python
import functools
import math

import jax
import jax.numpy as jnp
from jax import lax
from jax.experimental import pallas as pl
from jax.experimental.pallas import tpu as pltpu
from jax.sharding import PartitionSpec as P

HEAD_DIM = 64
NORM_EPS = 1e-06
GROUP_EPS = 0.00064
DECAY_TOP = math.exp(-0.5)
BLOCK = 64
VMEM_BYTES = 67043328
F32, BF16 = jnp.float32, jnp.bfloat16


def dot_dims(a, b, left, right):
    return lax.dot_general(
        a.astype(BF16), b.astype(BF16), (((left,), (right,)), ((), ())), preferred_element_type=F32
    )


def mm(a, b):
    return dot_dims(a, b, 1, 0)


def mmt(a, b):
    return dot_dims(a, b, 1, 1)


def tmm(a, b):
    return dot_dims(a, b, 0, 0)


def parts_of(x, count):
    found = []
    for _ in range(count):
        part = x.astype(BF16)
        found.append(part)
        x = x - part.astype(F32)
    return found


def head_ones(width):
    row = lax.broadcasted_iota(jnp.int32, (width, width), 0) // HEAD_DIM
    col = lax.broadcasted_iota(jnp.int32, (width, width), 1) // HEAD_DIM
    return (row == col).astype(F32)


def group_sum(x, ones, count=3):
    return sum(mm(part, ones) for part in parts_of(x, count))


def stack_heads(x):
    x = x.astype(BF16)
    count = x.shape[1] // HEAD_DIM
    if count == 1:
        return x
    lane = lax.broadcasted_iota(jnp.int32, (1, x.shape[1]), 1) // HEAD_DIM
    return jnp.concatenate([x * (lane == h).astype(F32).astype(BF16) for h in range(count)], axis=0)


def pack_heads(x):
    return sum(x[at : at + HEAD_DIM] for at in range(0, x.shape[0], HEAD_DIM))


def chain_inputs(keys, decay_pre, rate_pre, head_bias):
    k = keys.astype(F32)
    log_decay = -DECAY_TOP * jax.nn.sigmoid(head_bias[0:1] + decay_pre.astype(F32))
    rate = jax.nn.sigmoid(head_bias[1:2] + rate_pre.astype(F32))
    unit = k * lax.rsqrt(group_sum(k * k, head_ones(k.shape[1]), 2) + 1.0)
    return k, -unit, unit * rate, log_decay


def block_sums(log_decay):
    size = log_decay.shape[0]
    row = lax.broadcasted_iota(jnp.int32, (size, size), 0)
    col = lax.broadcasted_iota(jnp.int32, (size, size), 1)
    mask = ((row >= col) & (row // BLOCK == col // BLOCK)).astype(F32)
    return sum(mm(mask, part) for part in parts_of(log_decay, 3))


def pack_items(k, v, erase, write, log_decay, signs):
    items, ahead = [], block_sums(log_decay)
    for sign in signs:
        for at in range(0, k.shape[0], BLOCK):
            r = slice(at, at + BLOCK)
            total = ahead[at + BLOCK - 1 : at + BLOCK]
            cum = ahead[r]
            if not isinstance(sign, int):
                cum = jnp.where(sign > 0, cum, total - cum + log_decay[r])
            elif sign < 0:
                cum = total - cum + log_decay[r]
            items.append((sign, k[r], v[r], erase[r], write[r], log_decay[r], cum, total))
    return items


def signed_masks(sign, width):
    row = lax.broadcasted_iota(jnp.int32, (BLOCK, width), 0)
    col = lax.broadcasted_iota(jnp.int32, (BLOCK, width), 1) % BLOCK
    return (row - col) * sign > 0, (row - col) * sign >= 0


def beside(left, right):
    return jnp.concatenate([stack_heads(left), stack_heads(right)], axis=1)


def above(left, right):
    return jnp.concatenate([stack_heads(left), stack_heads(right)], axis=0)


def solve_maps(items, width):
    row = lax.broadcasted_iota(jnp.int32, (BLOCK, width), 0)
    col = lax.broadcasted_iota(jnp.int32, (BLOCK, width), 1) % BLOCK
    ones = head_ones(width)
    square = lax.broadcasted_iota(jnp.int32, (width, width), 0)
    unit = (square == lax.broadcasted_iota(jnp.int32, (width, width), 1)).astype(F32)
    one = (row == col).astype(F32)
    near = (row // 2 == col // 2) & (row != col)
    work = []
    for sign, k, v, erase, write, log_decay, cum, total in items:
        strict, _ = signed_masks(sign, width)
        growth = jnp.exp(-cum)
        item = {"es": (erase * jnp.exp(cum - log_decay)).astype(BF16), "v": v.astype(BF16), "cum": cum}
        item["wg"], item["kg"] = (write * growth).astype(BF16), (k * growth).astype(BF16)
        both = mmt(item["es"], above(item["wg"], item["kg"]))
        item["coupling"] = jnp.where(strict, both[:, :width], 0.0)
        item["feed"] = jnp.where(strict, both[:, width:], 0.0)
        tail = jnp.exp(total) * growth
        item["wt"], item["kt"] = (write * tail).astype(BF16), (k * tail).astype(BF16)
        item["diagonal"] = unit * jnp.exp(total)
        work.append(item)
    for item in work:
        item["x"] = one + jnp.where(near, item["coupling"], 0.0)
        item["fed"] = mm(item["feed"], stack_heads(item["v"]))
    size = 2
    while size < BLOCK:
        level = (row // (2 * size) == col // (2 * size)) & (row // size != col // size)
        for item in work:
            item["y"] = mm(jnp.where(level, item["coupling"], 0.0), stack_heads(item["x"]))
        for item in work:
            item["x"] = item["x"] + mm(item["x"], stack_heads(item["y"]))
        size *= 2
    for item in work:
        both = mm(item["x"], beside(item["es"], item["fed"])).astype(BF16)
        item["both"] = both
        item["response"], item["offset"] = both[:, :width], both[:, width:]
    for item in work:
        moved = tmm(item["both"], item["wt"])
        item["transfer"] = moved[:width] * ones + item["diagonal"]
        item["constant"] = (moved[width:] + tmm(item["v"], item["kt"])) * ones
    return work


MESH = pl.DeviceIdType.MESH


def advance(state, transfer, constant):
    high, low = parts_of(state, 2)
    both = mm(jnp.concatenate([high, low], axis=0), transfer)
    return both[:HEAD_DIM] + both[HEAD_DIM:] + constant


class Plan:
    def __init__(self, sp, tp, rows, context_rows, depth, local):
        self.sp, self.tp, self.chips = sp, tp, tp // 2
        self.block, self.context_rows = rows, context_rows
        self.rows = rows * tp
        self.depth, self.local = depth, local
        heads = local // HEAD_DIM
        self.width = (2 if heads % sp == 0 else 1) * HEAD_DIM
        self.packs = local // self.width
        self.units = 2 * self.packs // sp
        assert self.units in (1, 2) and self.units * sp == 2 * self.packs
        self.half = sp // 2
        self.fold = self.packs // self.half
        assert self.half * 2 == sp and self.fold * self.half == self.packs
        self.group = min(4, self.packs)
        self.groups = self.packs // self.group
        self.pieces = 2 if rows % 32 == 0 else 1
        self.chunk = max(128, local // sp)
        self.owners = local // self.chunk
        self.tile = 512
        self.out_tile = local
        self.out_tiles = depth // self.out_tile
        self.context_blocks = context_rows * sp // BLOCK


def remote(source, target, sent, taken, **peer):
    return pltpu.make_async_remote_copy(
        src_ref=source,
        dst_ref=target,
        send_sem=sent,
        recv_sem=taken,
        device_id=peer,
        device_id_type=MESH,
    )


def layer_kernel(
    plan,
    latent_hbm, context_hbm, condition_hbm, context_condition_hbm,
    shift_hbm, scale_hbm, gate_hbm, norm_gain_hbm,
    decay_down_hbm, decay_up_hbm, rate_down_hbm, rate_up_hbm, bias_hbm,
    query_hbm, key_hbm, value_hbm, branch_hbm, group_gain_hbm, out_hbm,
    updated_hbm,
    condition_v, norm_gain_ref, bias_ref, group_gain_ref, rows_v, context_v, wmod_v, wdown_v, wup_v, wbig_v,
    parts_v, part_in_v, vectors_v, gate_part_v, gate_in_v, gate_all_v, mod_v, inverse_v, normed_v,
    key_v, value_v, decay_v, rate_v, query_v, branch_v, bias_v,
    feature_out_v, feature_in_v, maps_out_v, maps_in_v, reads_q_v, base_v,
    saved_v, cum_v, first_v, transfer_v, constant_v,
    prefix_v, state_out_v, state_in_v, turn_out_v, turn_in_v, entry_out_v, entry_in_v, mixed_v,
    partial_v, pair_v, cross_out_v, cross_in_v, mixer_v,
    local_sem, row_s, row_r, relay_s, relay_r, part_s, part_r, vec_s, vec_r, gp_s, gp_r, gv_s, gv_r,
    feat_s, feat_r, map_s, map_r, st_s, st_r, turn_s, turn_r, ent_s, ent_r, pair_s, pair_r, cross_s, cross_r, store_sem,
):
    sp, tp, chips, width, packs, units = plan.sp, plan.tp, plan.chips, plan.width, plan.packs, plan.units
    depth, local, block = plan.depth, plan.local, plan.block
    half, fold, group, groups = plan.half, plan.fold, plan.group, plan.groups
    me_sp, me_tp = lax.axis_index("sp"), lax.axis_index("tp")
    chip, core = me_tp // 2, lax.rem(me_tp, 2)
    sibling = chip * 2 + 1 - core

    fetches = {}

    def fetch(name, at, source, target):
        copy = pltpu.make_async_copy(source, target, local_sem.at[at])
        copy.start()
        fetches[name] = copy

    def settle(ref, semaphore):
        remote(ref, ref, semaphore, semaphore, sp=me_sp, tp=me_tp).wait_recv()

    peers = sorted(range(1, sp), key=lambda d: (abs(d - half), d))

    barrier = pltpu.get_barrier_semaphore()
    everyone = [(a, b) for a in (*peers, 0) for b in reversed(range(tp)) if (a, b) != (0, 0)]
    greeted = [(a, b) for a, b in everyone if a == 0 or b == 0]
    for a, b in greeted:
        pl.semaphore_signal(
            barrier,
            inc=1,
            device_id={"sp": lax.rem(me_sp + a, sp), "tp": lax.rem(me_tp + b, tp)},
            device_id_type=MESH,
        )

    fetch("condition", 10, condition_hbm, condition_v.at[0])
    fetch("context_condition", 10, context_condition_hbm, condition_v.at[1])
    fetch("shift", 0, shift_hbm, wmod_v.at[0])
    fetch("scale", 1, scale_hbm, wmod_v.at[1])
    fetch("latent", 3, latent_hbm, rows_v.at[me_tp])
    fetch("context", 4, context_hbm, context_v)
    fetch("norm_gain", 13, norm_gain_hbm, norm_gain_ref)
    fetch("bias", 14, bias_hbm, bias_ref)
    fetch("group_gain", 15, group_gain_hbm, group_gain_ref)

    line = lax.broadcasted_iota(jnp.int32, (8, condition_v.shape[2]), 0)
    settle(condition_v, local_sem.at[10])
    values = jnp.where(line == 0, condition_v[0], jnp.where(line == 1, condition_v[1], 0.0))
    conditions = (values * jax.nn.sigmoid(values)).astype(BF16)
    for at, name in enumerate(("shift", "scale")):
        fetches[name].wait()
        share = mm(conditions, wmod_v[at])[0:2]
        for j in range(plan.owners):
            parts_v[j, 2 * at : 2 * at + 2] = share[:, j * plan.chunk : (j + 1) * plan.chunk]

    pl.semaphore_wait(barrier, len(greeted))

    def part_copy(d):
        peer = lax.rem(me_sp + d, sp)
        return peer, remote(
            parts_v.at[peer], part_in_v.at[d - 1], part_s.at[0], part_r.at[0], sp=peer, tp=me_tp
        )

    def gate_copy(d):
        peer = lax.rem(me_sp + d, sp)
        return remote(
            gate_part_v.at[peer], gate_in_v.at[d - 1], gp_s.at[0], gp_r.at[0], sp=peer, tp=me_tp
        )

    def when_owner(at, body):
        if plan.owners == sp:
            body()
        else:
            pl.when(at < plan.owners)(body)

    for d in peers:
        peer = lax.rem(me_sp + d, sp)
        when_owner(peer, lambda d=d: part_copy(d)[1].start())

    fetches["latent"].wait()

    def slot_of(d, c):
        return lax.rem(chip - d + chips, chips) * 2 + c

    piece = block // plan.pieces

    def row_copy(d, i, slot):
        part = rows_v.at[slot, pl.ds(i * piece, piece)]
        return remote(
            part, part, row_s.at[0], row_r.at[d - 1, i],
            sp=me_sp, tp=lax.rem(chip + d, chips) * 2 + core,
        )

    def relay_copy(d, i, c):
        part = rows_v.at[slot_of(d, c), pl.ds(i * piece, piece)]
        return remote(part, part, relay_s.at[0], relay_r.at[d], sp=me_sp, tp=sibling)

    row_copies = [row_copy(d, i, me_tp) for i in range(plan.pieces) for d in range(1, chips)]
    relay_copies = [relay_copy(d, i, core) for d in range(chips) for i in range(plan.pieces)]
    for copy in row_copies:
        copy.start()
    for i in range(plan.pieces):
        relay_copies[i].start()
    fetch("gate", 2, gate_hbm, wmod_v.at[2])
    fetch("decay_down", 5, decay_down_hbm, wdown_v.at[:, 0 : decay_down_hbm.shape[1]])
    fetch("rate_down", 5, rate_down_hbm, wdown_v.at[:, decay_down_hbm.shape[1] :])
    fetch("key", 7, key_hbm, wbig_v.at[0])
    fetch("value", 8, value_hbm, wbig_v.at[1])

    my_slot = me_tp * plan.owners + me_sp
    vector_copies = [
        remote(
            vectors_v.at[my_slot], vectors_v.at[my_slot], vec_s.at[0], vec_r.at[0],
            sp=lax.rem(me_sp + a, sp), tp=lax.rem(me_tp + b, tp),
        )
        for a, b in everyone
    ]

    def own_columns():
        total = parts_v[me_sp]
        settle(part_in_v, part_r.at[0])
        for d in range(1, sp):
            total = total + part_in_v[d - 1]
        vectors_v[my_slot] = total
        for copy in vector_copies:
            copy.start()

    when_owner(me_sp, own_columns)

    fetch("decay_up", 9, decay_up_hbm, wup_v.at[0])
    fetch("rate_up", 9, rate_up_hbm, wup_v.at[1])
    fetch("query", 11, query_hbm, wbig_v.at[2])
    fetch("branch", 12, branch_hbm, wbig_v.at[3])

    fetches["gate"].wait()
    share = mm(conditions, wmod_v[2])[0:1]
    for j in range(plan.owners):
        gate_part_v[j] = share[:, j * plan.chunk : (j + 1) * plan.chunk]
    for d in peers:
        when_owner(lax.rem(me_sp + d, sp), lambda d=d: gate_copy(d).start())

    def inverse_of(x):
        x = x.astype(F32)
        mean = jnp.sum(x * x, axis=-1, keepdims=True) * (1.0 / depth)
        return jnp.broadcast_to(lax.rsqrt(mean + NORM_EPS), (16, 128))

    fetches["context"].wait()
    for at in range(0, plan.context_rows, 16):
        inverse_v[(plan.rows + at) // 16] = inverse_of(context_v[at : at + 16])

    def block_inverse(slot):
        for at in range(0, block, 16):
            inverse_v[(slot * block + at) // 16] = inverse_of(rows_v[slot, at : at + 16])

    for name in ("norm_gain", "bias", "group_gain"):
        fetches[name].wait()
    for p in range(packs):
        bias_v[p] = bias_ref[:, p * width : (p + 1) * width]
    block_inverse(me_tp)
    settle(rows_v.at[sibling], relay_r.at[0])
    block_inverse(sibling)
    for i in range(plan.pieces):
        for d in range(1, chips):
            row_copy(d, i, slot_of(d, core)).wait_recv()
            relay_copies[d * plan.pieces + i].start()
    for d in range(1, chips):
        block_inverse(slot_of(d, core))
    for d in range(1, chips):
        settle(rows_v.at[slot_of(d, 1 - core)], relay_r.at[d])
        block_inverse(slot_of(d, 1 - core))

    def all_but_mine(ref, count, semaphore):
        if plan.owners == sp:
            settle(ref.at[pl.ds(0, count - 1)], semaphore)
        else:
            pl.when(me_sp < plan.owners)(lambda: settle(ref.at[pl.ds(0, count - 1)], semaphore))
            pl.when(me_sp >= plan.owners)(lambda: settle(ref.at[pl.ds(0, count)], semaphore))

    all_but_mine(vectors_v, tp * plan.owners, vec_r.at[0])

    for j in range(tp * plan.owners):
        c = slice(j * plan.chunk, (j + 1) * plan.chunk)
        tile = vectors_v[j]
        mod_v[0:2, c] = norm_gain_ref[:, c] * (1.0 + tile[2:4])
        mod_v[2:4, c] = tile[0:2]

    def modulate(read, group, which):
        inverse = inverse_v[group][:, 0:1]
        for at in range(0, depth, 512):
            c = slice(at, at + 512)
            x = read(c).astype(F32) * inverse * mod_v[which : which + 1, c] + mod_v[2 + which : 3 + which, c]
            normed_v[pl.ds(pl.multiple_of(group * 16, 16), 16), c] = x.astype(BF16)

    per = block // 16

    @pl.loop(0, plan.rows // 16, unroll=2)
    def _(g):
        slot, at = g // per, lax.rem(g, per) * 16
        modulate(lambda c: rows_v[slot, pl.ds(pl.multiple_of(at, 16), 16), c], g, 0)

    for at in range(0, plan.context_rows, 16):
        modulate(lambda c: context_v[at : at + 16, c], (plan.rows + at) // 16, 1)

    rank = decay_down_hbm.shape[1]
    settle(wdown_v, local_sem.at[5])
    settle(wup_v, local_sem.at[9])
    fetches["key"].wait()
    fetches["value"].wait()
    low = sum(
        jnp.dot(normed_v[:, c], wdown_v[c], preferred_element_type=F32)
        for c in (slice(0, depth // 2), slice(depth // 2, depth))
    )
    gate_copies = [
        remote(
            gate_all_v.at[my_slot], gate_all_v.at[my_slot], gv_s.at[0], gv_r.at[0],
            sp=lax.rem(me_sp + a, sp), tp=lax.rem(me_tp + b, tp),
        )
        for a, b in everyone
    ]

    def own_gate():
        total = gate_part_v[me_sp]
        settle(gate_in_v, gp_r.at[0])
        for d in range(1, sp):
            total = total + gate_in_v[d - 1]
        gate_all_v[my_slot] = total
        for copy in gate_copies:
            copy.start()

    def spread(found, at, target, kind):
        found = found.astype(BF16)
        for p in range(found.shape[1] // width):
            piece = found[:, p * width : (p + 1) * width]
            target[at // width + p] = piece[: plan.rows]
            if kind is not None:
                feature_out_v[at // width + p, kind] = piece[plan.rows :]

    def project(which, rows, target, kind, tiles):
        for at in tiles:
            found = jnp.dot(
                normed_v[0:rows], wbig_v[which, :, at : at + plan.tile], preferred_element_type=F32
            )
            spread(found, at, target, kind)

    def pack_of(d):
        return (d * units) // 2

    def feature_part(at, i):
        return at.at[(pl.ds(2, 2), pl.ds(0, 1), pl.ds(1, 1))[i]]

    def feature_copy(d, i):
        peer = lax.rem(me_sp + d, sp)
        return remote(
            feature_part(feature_out_v.at[pack_of(peer)], i), feature_part(feature_in_v.at[me_sp], i),
            feat_s.at[0], feat_r.at[0], sp=peer, tp=me_tp,
        )

    everything = plan.rows + plan.context_rows
    tiles = list(range(0, local, plan.tile))
    project(0, everything, key_v, 0, tiles[:1])
    decay_low = jnp.tanh(low[:, :rank]).astype(BF16)
    rate_low = low[:, rank:].astype(BF16)

    for name, lhs, which, target, kind in (
        ("decay_up", decay_low, 0, decay_v, 2),
        ("rate_up", rate_low, 1, rate_v, 3),
    ):
        for at in range(0, local, plan.tile):
            found = jnp.dot(lhs, wup_v[which, :, at : at + plan.tile], preferred_element_type=F32)
            spread(found, at, target, kind)
    for d in peers:
        feature_copy(d, 0).start()
    project(0, everything, key_v, 0, tiles[1:])
    for d in peers:
        feature_copy(d, 1).start()
    for j in range(plan.out_tiles):
        fetch("out", 6, out_hbm.at[:, j * local : (j + 1) * local], wbig_v.at[0, j * local : (j + 1) * local])
    project(1, everything, value_v, 1, tiles)
    for d in peers:
        feature_copy(d, 2).start()
    feature_in_v[me_sp] = feature_out_v[pack_of(me_sp)]
    when_owner(me_sp, own_gate)

    side, index = me_sp // half, lax.rem(me_sp, half)
    blocks = plan.rows // BLOCK

    def map_copy(p):
        owner, slot = p // fold, lax.rem(p, fold)
        d = lax.rem(owner - index + half, half)
        return d, remote(
            maps_out_v.at[p], maps_in_v.at[index, slot], map_s.at[0], map_r.at[0],
            sp=side * half + owner, tp=me_tp,
        )

    def latent_maps(s):
        at = [lax.rem((index + 1) * fold + s * group + i, packs) for i in range(group)]
        items = []
        for p in at:
            k, erase, write, log_decay = chain_inputs(key_v[p], decay_v[p], rate_v[p], bias_v[p])
            items += pack_items(k, value_v[p], erase, write, log_decay, (1, -1))
        found = solve_maps(items, width)
        for i, p in enumerate(at):
            for way in (0, 1):
                mine = found[(i * 2 + way) * blocks : (i * 2 + way + 1) * blocks]
                carried = None
                for b in range(blocks) if way == 0 else reversed(range(blocks)):
                    item = mine[b]
                    transfer, constant = item["transfer"], item["constant"]
                    if carried is not None:
                        first_v[p, way, b, :width] = carried[0].astype(BF16)
                        first_v[p, way, b, width:] = carried[1].astype(BF16)
                        both = mm(jnp.concatenate(carried, axis=0), transfer)
                        transfer, constant = both[:width], both[width:] + constant
                    carried = (transfer, constant)
                    for kind, name in enumerate(("wg", "kg", "response", "offset")):
                        saved_v[p, way, b, kind] = item[name]
                    cum_v[p, way, b] = item["cum"]
                maps_out_v[p, way, 0] = pack_heads(carried[0]).astype(BF16)
                maps_out_v[p, way, 1] = pack_heads(carried[1]).astype(BF16)
            d, copy = map_copy(p)

            @pl.when(d != 0)
            def _(copy=copy):
                copy.start()

    pl.loop(0, groups)(latent_maps)
    for i in range(fold):
        maps_in_v[index, i] = maps_out_v[index * fold + i]

    settle(feature_in_v.at[pl.ds(0, sp - 1)], feat_r.at[0])
    keys, vals, decay_pre, rate_pre = (
        jnp.concatenate([feature_in_v[at, kind] for at in range(sp)], axis=0) for kind in range(4)
    )
    held = pack_of(me_sp)
    k, erase, write, log_decay = chain_inputs(keys, decay_pre, rate_pre, bias_v[held])
    count = plan.context_blocks
    if units == 2:
        ways = (0, 1)
    else:
        ways = (lax.rem(me_sp, 2),)
    found = solve_maps(pack_items(k, vals, erase, write, log_decay, [1 - 2 * way for way in ways]), width)

    def state_copy(u):
        target = ways[u] * half + held // fold
        slot = lax.rem(held, fold)
        return target, slot, remote(
            state_out_v.at[u], state_in_v.at[slot], st_s.at[u], st_r.at[slot], sp=target, tp=me_tp
        )

    for u in range(units):
        mine = found[u * count : (u + 1) * count]
        if units == 2:
            order = mine if u == 0 else mine[::-1]
            state = pack_heads(order[0]["constant"])
            for item in order[1:]:
                state = advance(state, item["transfer"], pack_heads(item["constant"]))
        else:
            for b, item in enumerate(mine):
                transfer_v[b] = item["transfer"].astype(BF16)
                constant_v[b] = pack_heads(item["constant"])
            state = constant_v[jnp.where(ways[0] == 1, count - 1, 0)]
            for step in range(1, count):
                b = jnp.where(ways[0] == 1, count - 1 - step, step)
                state = advance(state, transfer_v[b], constant_v[b])
        state_out_v[u] = state.astype(BF16)
        target, slot, copy = state_copy(u)

        @pl.when(target != me_sp)
        def _(copy=copy):
            copy.start()

        @pl.when(target == me_sp)
        def _(u=u, slot=slot):
            state_in_v[slot] = state_out_v[u]

    fetches["query"].wait()
    project(2, plan.rows, query_v, None, tiles)

    def latent_queries(s):
        jobs = []
        for i in range(group):
            p = s * group + i
            for way in (0, 1):
                _, inclusive = signed_masks(1 - 2 * way, width)
                for b in range(blocks):
                    q = query_v[p, b * BLOCK : (b + 1) * BLOCK].astype(F32) * jnp.exp(cum_v[p, way, b])
                    jobs.append({"p": p, "way": way, "b": b, "q": q, "mask": inclusive})
        for job in jobs:
            p, way, b = job["p"], job["way"], job["b"]
            both = mmt(job["q"], above(saved_v[p, way, b, 0], saved_v[p, way, b, 1]))
            job["aw"] = jnp.where(job["mask"], both[:, :width], 0.0)
            job["ak"] = jnp.where(job["mask"], both[:, width:], 0.0)
        for job in jobs:
            p, way, b = job["p"], job["way"], job["b"]
            both = mm(job["aw"], beside(saved_v[p, way, b, 2], saved_v[p, way, b, 3]))
            job["query"] = job["q"] + both[:, :width]
            fed = mm(job["ak"], stack_heads(value_v[p, b * BLOCK : (b + 1) * BLOCK]))
            job["base"] = both[:, width:] + fed
        for job in jobs:
            p, way, b = job["p"], job["way"], job["b"]
            if b != (0 if way == 0 else blocks - 1):
                both = mmt(job["query"], first_v[p, way, b])
                job["query"] = both[:, :width]
                job["base"] = job["base"] + both[:, width:]
            reads_q_v[p, way, b * BLOCK : (b + 1) * BLOCK] = job["query"].astype(BF16)
        for i in range(group):
            mine = jobs[i * 2 * blocks : (i + 1) * 2 * blocks]
            for b in range(blocks):
                base_v[s * group + i, b * BLOCK : (b + 1) * BLOCK] = mine[b]["base"] + mine[blocks + b]["base"]

    def entry_copy(stage, way, at):
        return remote(
            entry_out_v.at[stage, at], entry_in_v.at[way, pl.ds(index * fold, fold)],
            ent_s.at[stage], ent_r.at[stage], sp=side * half + at, tp=me_tp,
        )

    def place(way, step):
        return jnp.where(way == 0, step, half - 1 - step)

    def compose_maps(way):
        for i in range(fold):
            found = maps_in_v[place(way, 0), i, way]
            both = jnp.concatenate([found[0].astype(F32), found[1].astype(F32)], axis=0)
            prefix_v[way, i, 0] = both.astype(BF16)
            for step in range(1, half):
                found = maps_in_v[place(way, step), i, way]
                both = mm(both, stack_heads(found[0]))
                both = jnp.concatenate([both[:HEAD_DIM], both[HEAD_DIM:] + found[1].astype(F32)], axis=0)
                prefix_v[way, i, step] = both.astype(BF16)

    def moved(way, i, step, state):
        found = prefix_v[way, i, step]
        return advance(state, stack_heads(found[:HEAD_DIM]), found[HEAD_DIM:].astype(F32))

    def fold_maps(stage, way, start):
        states = [start[i].astype(F32) for i in range(fold)]
        for i in range(fold):
            entry_out_v[stage, place(way, 0), i] = start[i]
        for step in range(1, half):
            for i in range(fold):
                entry_out_v[stage, place(way, step), i] = moved(way, i, step - 1, states[i]).astype(BF16)
        for d in range(1, half):
            entry_copy(stage, way, lax.rem(index + d, half)).start()
        for i in range(fold):
            entry_in_v[way, index * fold + i] = entry_out_v[stage, index, i]

    def entries_arrived(stage, way):
        settle(entry_in_v.at[way, pl.ds(0, (half - 1) * fold)], ent_r.at[stage])

    settle(maps_in_v.at[pl.ds(0, half - 1)], map_r.at[0])
    for way in (0, 1):
        compose_maps(way)
    for i in range(fold):
        p = index * fold + i

        @pl.when((2 * p + side) // units != me_sp)
        def _(i=i):
            remote(
                state_out_v.at[0], state_in_v.at[i], st_s.at[0], st_r.at[i], sp=me_sp, tp=me_tp
            ).wait_recv()

    for i in range(fold):
        turn_out_v[i] = moved(side, i, half - 1, state_in_v[i].astype(F32)).astype(BF16)
    turn = remote(
        turn_out_v, turn_in_v, turn_s.at[0], turn_r.at[0], sp=(1 - side) * half + index, tp=me_tp
    )
    turn.start()
    fold_maps(0, side, state_in_v)
    pl.loop(0, groups)(latent_queries)

    turn.wait_recv()
    fold_maps(1, 1 - side, turn_in_v)
    fetches["branch"].wait()
    project(3, plan.rows, branch_v, None, tiles)

    entries_arrived(0, side)
    for p in range(packs):
        base_v[p] = base_v[p] + mmt(reads_q_v[p, side], stack_heads(entry_in_v[side, p]))
    entries_arrived(1, 1 - side)

    ones = head_ones(width)
    pair_rows = 2 * block

    def mixed_rows(e):
        at = pl.multiple_of(lax.rem(chip + e, chips) * pair_rows, pair_rows)
        r = pl.ds(at, pair_rows)
        found = [
            base_v[p, r] + mmt(reads_q_v[p, 1 - side, r], stack_heads(entry_in_v[1 - side, p]))
            for p in range(packs)
        ]
        away = [x - group_sum(x, ones, 2) * (1.0 / HEAD_DIM) for x in found]
        variance = [group_sum(x * x, ones, 2) * (1.0 / HEAD_DIM) for x in away]
        for p in range(packs):
            c = slice(p * width, (p + 1) * width)
            gates = branch_v[p, r].astype(F32)
            mixed_v[:, c] = (
                away[p] * lax.rsqrt(variance[p] + GROUP_EPS)
                * group_gain_ref[:, c] * (gates * jax.nn.sigmoid(gates))
            ).astype(BF16)

    def pair_copy(e, j):
        return remote(
            partial_v.at[e, j, 1 - core], pair_v.at[e, j], pair_s.at[0], pair_r.at[(e - 1) * plan.out_tiles + j if e else (chips - 1) * plan.out_tiles],
            sp=me_sp, tp=sibling,
        )

    def cross_copy(e, j):
        return remote(
            cross_out_v.at[e - 1, j], cross_in_v.at[e - 1, j], cross_s.at[0], cross_r.at[e - 1, j],
            sp=me_sp, tp=lax.rem(chip + e, chips) * 2 + core,
        )

    def out_copy(j):
        return pltpu.make_async_copy(
            mixer_v.at[:, j * local : (j + 1) * local], updated_hbm.at[:, j * local : (j + 1) * local], store_sem.at[0]
        )

    settle(wbig_v.at[0], local_sem.at[6])
    for e in [*range(1, chips), 0]:
        mixed_rows(e)
        for j in range(plan.out_tiles):
            found = mm(mixed_v[...], wbig_v[0, j * local : (j + 1) * local]).astype(BF16)
            for i in range(2):
                partial_v[e, j, i] = found[i * block : (i + 1) * block]
            pair_copy(e, j).start()
        if e > 0:
            for j in range(plan.out_tiles):
                pair_copy(e, j).wait_recv()
                cross_out_v[e - 1, j] = (
                    partial_v[e, j, core].astype(F32) + pair_v[e, j].astype(F32)
                ).astype(BF16)
                cross_copy(e, j).start()
    all_but_mine(gate_all_v, tp * plan.owners, gv_r.at[0])
    settle(pair_v.at[0], pair_r.at[(chips - 1) * plan.out_tiles])
    square = jnp.zeros((block, 1), F32)
    totals = []
    for j in range(plan.out_tiles):
        total = partial_v[0, j, core].astype(F32) + pair_v[0, j].astype(F32)
        for e in range(1, chips):
            cross_copy(e, j).wait_recv()
            total = total + cross_in_v[e - 1, j].astype(F32)
        total = total.astype(BF16)
        mixer_v[:, j * local : (j + 1) * local] = total
        total = total.astype(F32)
        square = square + jnp.sum(total * total, axis=-1, keepdims=True)
    inverse = lax.rsqrt(square * (1.0 / depth) + NORM_EPS)
    per_tile = local // plan.chunk
    for j in range(plan.out_tiles):
        for i in range(j * per_tile, (j + 1) * per_tile):
            c = slice(i * plan.chunk, (i + 1) * plan.chunk)
            mixer_v[:, c] = (
                rows_v[me_tp, :, c].astype(F32) + gate_all_v[i] * (mixer_v[:, c].astype(F32) * inverse)
            ).astype(BF16)
        out_copy(j).start()

    all_but_mine(parts_v, plan.owners, part_s.at[0])
    all_but_mine(gate_part_v, plan.owners, gp_s.at[0])
    settle(rows_v.at[pl.ds(0, chips - 1)], row_s.at[0])
    settle(rows_v.at[pl.ds(0, chips)], relay_s.at[0])

    def vectors_left():
        left = len(everyone)
        for ref, semaphore in ((vectors_v, vec_s.at[0]), (gate_all_v, gv_s.at[0])):
            whole, rest = left // ref.shape[0], left % ref.shape[0]
            for _ in range(whole):
                settle(ref, semaphore)
            if rest:
                settle(ref.at[pl.ds(0, rest)], semaphore)

    when_owner(me_sp, vectors_left)
    settle(feature_in_v.at[pl.ds(0, sp - 1)], feat_s.at[0])
    settle(maps_in_v.at[pl.ds(0, half - 1)], map_s.at[0])
    for stage in (0, 1):
        settle(entry_in_v.at[0, pl.ds(0, (half - 1) * fold)], ent_s.at[stage])
    for u in range(units):
        target, _, copy = state_copy(u)

        @pl.when(target != me_sp)
        def _(copy=copy):
            copy.wait_send()

    turn.wait_send()
    settle(pair_v, pair_s.at[0])
    settle(cross_out_v, cross_s.at[0])
    settle(mixer_v, store_sem.at[0])


def on_device(
    latent,
    context,
    condition,
    context_condition,
    shift_weight,
    scale_weight,
    gate_weight,
    norm_gain,
    decay_down,
    decay_up,
    rate_down,
    rate_up,
    head_bias,
    query_weight,
    key_weight,
    value_weight,
    branch_weight,
    group_gain,
    out_weight,
):
    sp, tp = lax.axis_size("sp"), lax.axis_size("tp")
    block, depth = latent.shape
    local = query_weight.shape[1]
    plan = Plan(sp, tp, block, context.shape[0], depth, local)
    width, packs, units, chips = plan.width, plan.packs, plan.units, plan.chips
    rows, crows, tiles = plan.rows, plan.context_rows, plan.out_tiles
    half, fold, blocks = plan.half, plan.fold, rows // BLOCK
    rank = decay_down.shape[1]
    hbm = pl.BlockSpec(memory_space=pltpu.HBM)
    scratch = [
        ((2, 1, condition.shape[0]), F32),
        ((1, depth), F32),
        ((2, local), F32),
        ((1, local), F32),
        ((tp, block, depth), BF16),
        ((crows, depth), BF16),
        ((3, *shift_weight.shape), BF16),
        ((depth, 2 * rank), BF16),
        ((2, rank, local), BF16),
        ((4, depth, local), BF16),
        ((plan.owners, 4, plan.chunk), F32),
        ((sp - 1, 4, plan.chunk), F32),
        ((tp * plan.owners, 4, plan.chunk), F32),
        ((plan.owners, 1, plan.chunk), F32),
        ((sp - 1, 1, plan.chunk), F32),
        ((tp * plan.owners, 1, plan.chunk), F32),
        ((8, depth), F32),
        (((rows + crows) // 16, 16, 128), F32),
        ((rows + crows, depth), BF16),
        ((packs, rows, width), BF16),
        ((packs, rows, width), BF16),
        ((packs, rows, width), BF16),
        ((packs, rows, width), BF16),
        ((packs, rows, width), BF16),
        ((packs, rows, width), BF16),
        ((packs, 2, width), F32),
        ((packs, 4, crows, width), BF16),
        ((sp, 4, crows, width), BF16),
        ((packs, 2, 2, HEAD_DIM, width), BF16),
        ((half, fold, 2, 2, HEAD_DIM, width), BF16),
        ((packs, 2, rows, width), BF16),
        ((packs, rows, width), F32),
        ((packs, 2, blocks, 4, BLOCK, width), BF16),
        ((packs, 2, blocks, BLOCK, width), F32),
        ((packs, 2, blocks, 2 * width, width), BF16),
        ((plan.context_blocks, width, width), BF16),
        ((plan.context_blocks, HEAD_DIM, width), F32),
        ((2, fold, half, 2 * HEAD_DIM, width), BF16),
        ((units, HEAD_DIM, width), BF16),
        ((fold, HEAD_DIM, width), BF16),
        ((fold, HEAD_DIM, width), BF16),
        ((fold, HEAD_DIM, width), BF16),
        ((2, half, fold, HEAD_DIM, width), BF16),
        ((2, packs, HEAD_DIM, width), BF16),
        ((2 * block, local), BF16),
        ((chips, tiles, 2, block, plan.out_tile), BF16),
        ((chips, tiles, block, plan.out_tile), BF16),
        ((chips - 1, tiles, block, plan.out_tile), BF16),
        ((chips - 1, tiles, block, plan.out_tile), BF16),
        ((block, depth), BF16),
    ]
    pieces = plan.pieces
    semaphores = [
        (16,), (1,), (chips - 1, pieces), (1,), (chips,),
        (1,), (1,), (1,), (1,), (1,), (1,), (1,), (1,),
        (1,), (1,), (1,), (1,), (units,), (fold,), (1,), (1,), (2,), (2,),
        (1,), ((chips - 1) * tiles + 1,), (1,), (chips - 1, tiles), (1,),
    ]
    return pl.pallas_call(
        functools.partial(layer_kernel, plan),
        in_specs=[hbm] * 19,
        out_specs=hbm,
        out_shape=jax.ShapeDtypeStruct(latent.shape, BF16),
        scratch_shapes=[pltpu.VMEM(shape, kind) for shape, kind in scratch]
        + [pltpu.SemaphoreType.DMA(shape) for shape in semaphores],
        compiler_params=pltpu.CompilerParams(
            collective_id=0, has_side_effects=True, vmem_limit_bytes=VMEM_BYTES
        ),
        name="layer",
    )(
        latent, context, condition.reshape(1, -1), context_condition.reshape(1, -1),
        shift_weight, scale_weight, gate_weight, norm_gain.reshape(1, -1),
        decay_down, decay_up, rate_down, rate_up, head_bias,
        query_weight, key_weight, value_weight, branch_weight, group_gain.reshape(1, -1), out_weight,
    )


def solution(mesh):
    placed = (
        P(("sp", "tp"), None),
        P("sp", None),
        P("sp"),
        P("sp"),
        P("sp", "tp"),
        P("sp", "tp"),
        P("sp", "tp"),
        P(),
        P(),
        P(None, "tp"),
        P(),
        P(None, "tp"),
        P(None, "tp"),
        P(None, "tp"),
        P(None, "tp"),
        P(None, "tp"),
        P(None, "tp"),
        P("tp"),
        P("tp", None),
    )
    return jax.shard_map(
        on_device, mesh=mesh, in_specs=placed, out_specs=P(("sp", "tp"), None), check_vma=False
    )
```
